32 devices in a mesh: sp: 16 (over z, y, x), tp: 2 (over core).
Axes of the slice: x: 2, y: 2, z: 4, core: 2. Of those that a mesh axis runs over, the one named last changes fastest.
Arguments:
- tokens: bfloat16 [6144, 2048], P('sp', 'tp'), may hold values from -6 to 6
- input_gain: float32 [2048], replicated, may hold values from 0.1 to 1.9
- query_weight: bfloat16 [2048, 1024], P(None, 'tp'), may hold values from -0.5 to 0.5
- query_rot_weight: bfloat16 [2048, 512], P(None, 'tp'), may hold values from -0.125 to 0.125
- kv_down: bfloat16 [2048, 256], replicated, may hold values from -0.5 to 0.5
- rot_down: bfloat16 [2048, 32], replicated, may hold values from -0.125 to 0.125
- kv_gain: float32 [256], replicated, may hold values from 0.1 to 1.9
- key_up: bfloat16 [256, 1024], P(None, 'tp'), may hold values from -0.5 to 0.5
- value_up: bfloat16 [256, 1024], P(None, 'tp'), may hold values from -4 to 4
- conv_value_weight: bfloat16 [2048, 1024], P(None, 'tp'), may hold values from -0.125 to 0.125
- conv_gate_weight: bfloat16 [2048, 1024], P(None, 'tp'), may hold values from -0.125 to 0.125
- conv_taps: float32 [31, 1024], P(None, 'tp'), may hold values from -8 to 8
- conv_ln_gain: float32 [1024], P('tp'), may hold values from 0.1 to 1.9
- conv_ln_bias: float32 [1024], P('tp'), may hold values from -3 to 3
- att_out_gain: float32 [1024], P('tp'), may hold values from 0.1 to 1.9
- conv_out_gain: float32 [1024], P('tp'), may hold values from 0.1 to 1.9
- att_out_weight: bfloat16 [1024, 2048], P('tp'), may hold values from -0.125 to 0.125
- conv_out_weight: bfloat16 [1024, 2048], P('tp'), may hold values from -0.125 to 0.125
Outputs:
- mixed: bfloat16 [6144, 2048], P('sp', 'tp')
The draws below stay inside these ranges and needn't reach their ends.
All inputs are finite; a program needn't handle non-finite values.
Results may differ from the reference program's by a relative error of at most 0.017.
Values may be sent and summed in bfloat16 or wider, within the bound.
No kernel may reach another device: no remote copies, remote signals or barrier semaphores. Data moves between devices by JAX's collectives and lax.ppermute only.
A program may use at most 128 MiB of HBM per device.

```python
import math
import jax
import jax.numpy as jnp
from jax import lax

D_MODEL = 2048
HEADS = 16
NOPE_DIM = 64
ROT_DIM = 32
VALUE_DIM = 64
KV_RANK = 256
CONV_CH = 1024
KERNEL = 31
TOKENS = 6144
ATT_WIDTH = 1024
N_TP = 2


def latent_weights(key):
    down_map = jax.random.normal(jax.random.fold_in(key, 101), (D_MODEL, KV_RANK), jnp.float32) / math.sqrt(D_MODEL)
    upward = jax.random.normal(jax.random.fold_in(key, 102), (KV_RANK, HEADS * NOPE_DIM), jnp.float32) / math.sqrt(KV_RANK)
    return (jnp.clip(down_map, -0.5, 0.5), jnp.clip(upward, -0.5, 0.5))


def rising_scales(key, entries):
    position = jnp.arange(entries, dtype=jnp.float32) / max(entries - 1, 1)
    jitter = jax.random.uniform(key, (entries,), jnp.float32)
    return 10.0 ** (0.5 * position + 0.5 * jitter - 0.5)


def draw_tokens(key, part):
    base_draw = jax.random.normal(jax.random.fold_in(key, 1), (TOKENS, D_MODEL), jnp.float32)
    return jnp.clip(base_draw, -6.0, 6.0).astype(jnp.bfloat16)


def draw_query_weight(key, part):
    base_draw = jax.random.normal(jax.random.fold_in(key, 104), (D_MODEL, HEADS * NOPE_DIM), jnp.float32) / math.sqrt(D_MODEL)
    return jnp.clip(base_draw, -0.5, 0.5).astype(jnp.bfloat16)


def draw_kv_down(key, part):
    return latent_weights(key)[0].astype(jnp.bfloat16)


def draw_key_up(key, part):
    return latent_weights(key)[1].astype(jnp.bfloat16)


def draw_value_up(key, part):
    base_draw = jax.random.normal(jax.random.fold_in(key, 201), (KV_RANK, HEADS * VALUE_DIM), jnp.float32) / math.sqrt(KV_RANK)
    scales = jnp.repeat(rising_scales(jax.random.fold_in(key, 202), HEADS), VALUE_DIM)
    return jnp.clip(base_draw * scales[None, :], -4.0, 4.0).astype(jnp.bfloat16)


def draw_conv_taps(key, part):
    base_draw = jax.random.normal(jax.random.fold_in(key, 301), (KERNEL, CONV_CH), jnp.float32) / math.sqrt(KERNEL)
    scales = rising_scales(jax.random.fold_in(key, 302), CONV_CH)
    return jnp.clip(base_draw * scales[None, :], -8.0, 8.0).astype(jnp.float32)


def steps_of(stream_key, dims, shards, least, largest):
    def one(dim, parts):
        heights = jax.random.uniform(jax.random.fold_in(jax.random.fold_in(stream_key, 6), dim), (parts,), jnp.float32, least / len(shards), largest / len(shards))
        return jnp.repeat(jnp.exp(heights), dims[dim] // parts).reshape((-1,) + (1,) * (len(dims) - dim - 1))

    level = one(*shards[0])
    for cut in shards[1:]:
        level = level * one(*cut)
    return level


def centred(own_key, dims, width, limit, split=(), held_as=jnp.bfloat16):
    values = width * jax.random.normal(own_key, dims, jnp.float32)
    if split:
        values = values * steps_of(own_key, dims, split, -0.22, 0.18)
    return jnp.clip(values, -limit, limit).astype(held_as)


def setup_inputs(seed: int = 0) -> dict:
    key_of = jax.random.split(jax.random.key(seed), 19)
    tokens = draw_tokens(jax.random.fold_in(key_of[18], 71), 0)
    input_gain = jnp.clip(1.0 + 0.18 * jax.random.normal(key_of[1], (D_MODEL,), jnp.float32), 0.1, 1.9)
    query_weight = draw_query_weight(jax.random.fold_in(key_of[18], 71), 0)
    query_rot_weight = centred(key_of[3], (D_MODEL, HEADS * ROT_DIM), D_MODEL ** -0.5, 0.125, ((1, 2),))
    kv_down = draw_kv_down(jax.random.fold_in(key_of[18], 71), 0)
    rot_down = centred(key_of[5], (D_MODEL, ROT_DIM), D_MODEL ** -0.5, 0.125)
    kv_gain = jnp.clip(1.0 + 0.18 * jax.random.normal(key_of[6], (KV_RANK,), jnp.float32), 0.1, 1.9)
    key_up = draw_key_up(jax.random.fold_in(key_of[18], 71), 0)
    value_up = draw_value_up(jax.random.fold_in(key_of[18], 71), 0)
    conv_value_weight = centred(key_of[9], (D_MODEL, CONV_CH), D_MODEL ** -0.5, 0.125, ((1, 2),))
    conv_gate_weight = centred(key_of[10], (D_MODEL, CONV_CH), D_MODEL ** -0.5, 0.125, ((1, 2),))
    conv_taps = draw_conv_taps(jax.random.fold_in(key_of[18], 71), 0)
    conv_ln_gain = jnp.clip(1.0 + 0.18 * jax.random.normal(key_of[12], (CONV_CH,), jnp.float32), 0.1, 1.9)
    conv_ln_bias = centred(key_of[13], (CONV_CH,), 0.5, 3.0, ((0, 2),), jnp.float32)
    att_out_gain = jnp.clip(1.0 + 0.18 * jax.random.normal(key_of[14], (ATT_WIDTH,), jnp.float32), 0.1, 1.9)
    conv_out_gain = jnp.clip(1.0 + 0.18 * jax.random.normal(key_of[15], (CONV_CH,), jnp.float32), 0.1, 1.9)
    att_out_weight = centred(key_of[16], (ATT_WIDTH, D_MODEL), (ATT_WIDTH + CONV_CH) ** -0.5, 0.125, ((0, 2),))
    conv_out_weight = centred(key_of[17], (CONV_CH, D_MODEL), (ATT_WIDTH + CONV_CH) ** -0.5, 0.125, ((0, 2),))
    return {"tokens": tokens, "input_gain": input_gain, "query_weight": query_weight, "query_rot_weight": query_rot_weight, "kv_down": kv_down, "rot_down": rot_down, "kv_gain": kv_gain, "key_up": key_up, "value_up": value_up, "conv_value_weight": conv_value_weight, "conv_gate_weight": conv_gate_weight, "conv_taps": conv_taps, "conv_ln_gain": conv_ln_gain, "conv_ln_bias": conv_ln_bias, "att_out_gain": att_out_gain, "conv_out_gain": conv_out_gain, "att_out_weight": att_out_weight, "conv_out_weight": conv_out_weight}


norm_eps = 1e-06
rope_base = 10000.0

def lifted(array):
    return lax.optimization_barrier(array).astype(jnp.float32)

def rotary_tables(positions, half_dim):
    frequency = rope_base ** (-jnp.arange(half_dim, dtype=jnp.float32) / half_dim)
    angles = positions.astype(jnp.float32)[:, None] * frequency[None, :]
    return (jnp.cos(angles), jnp.sin(angles))

def rotate_half(values, cos_table, sine_table):
    half_dim = cos_table.shape[-1]
    front_half = values[..., :half_dim]
    back_half = values[..., half_dim:]
    return jnp.concatenate([front_half * cos_table - back_half * sine_table, back_half * cos_table + front_half * sine_table], axis=-1)

def reference(tokens, input_gain, query_weight, query_rot_weight, kv_down, rot_down, kv_gain, key_up, value_up, conv_value_weight, conv_gate_weight, conv_taps, conv_ln_gain, conv_ln_bias, att_out_gain, conv_out_gain, att_out_weight, conv_out_weight):
    tokens_wide = tokens.astype(jnp.float32)
    row_scale = lax.rsqrt(lax.optimization_barrier(jnp.mean(tokens_wide * tokens_wide, axis=1, keepdims=True)) + norm_eps)
    scaled = (tokens_wide * input_gain[None, :]).astype(jnp.bfloat16)

    def project(weight):
        return jnp.dot(scaled.astype(jnp.float32), weight.astype(jnp.float32), preferred_element_type=jnp.float32)
    positions = jnp.arange(TOKENS, dtype=jnp.int32)
    cos_table, sine_table = rotary_tables(positions, ROT_DIM // 2)
    queries = (project(query_weight) * row_scale).astype(jnp.bfloat16).reshape(TOKENS, HEADS, NOPE_DIM)
    query_rot = rotate_half((project(query_rot_weight) * row_scale).reshape(TOKENS, HEADS, ROT_DIM), cos_table[:, None, :], sine_table[:, None, :]).astype(jnp.bfloat16)
    latent_raw = project(kv_down)
    latent = (latent_raw * lax.rsqrt(lax.optimization_barrier(jnp.mean(latent_raw * latent_raw, axis=1, keepdims=True)) + norm_eps) * kv_gain[None, :]).astype(jnp.bfloat16)
    key_rot = rotate_half(project(rot_down) * row_scale, cos_table, sine_table).astype(jnp.bfloat16)
    keys = jnp.dot(latent.astype(jnp.float32), key_up.astype(jnp.float32), preferred_element_type=jnp.float32).astype(jnp.bfloat16).reshape(TOKENS, HEADS, NOPE_DIM)
    values = jnp.dot(latent.astype(jnp.float32), value_up.astype(jnp.float32), preferred_element_type=jnp.float32).astype(jnp.bfloat16).reshape(TOKENS, HEADS, VALUE_DIM)
    queries_heads = jnp.transpose(lifted(queries), (1, 0, 2))
    qrot_heads = jnp.transpose(lifted(query_rot), (1, 0, 2))
    keys_heads = jnp.transpose(lifted(keys), (1, 0, 2))
    values_heads = jnp.transpose(lifted(values), (1, 0, 2))
    krot_wide = lifted(key_rot)
    inv_scale = 1.0 / math.sqrt(NOPE_DIM + ROT_DIM)
    block_len = min(512, TOKENS)
    pieces = []
    for block_idx in range(TOKENS // block_len):
        row_low = block_idx * block_len
        row_high = row_low + block_len
        key_pos = jnp.arange(row_high, dtype=jnp.int32)
        query_pos = jnp.arange(row_low, row_high, dtype=jnp.int32)
        visible = key_pos[None, :] <= query_pos[:, None]
        krot_part = krot_wide[:row_high]

        def one_head(members):
            query_head, qrot_head, key_head, value_head = members
            scores = (jnp.dot(query_head, key_head.T) + jnp.dot(qrot_head, krot_part.T)) * inv_scale
            row_max = lax.optimization_barrier(jnp.max(jnp.where(visible, scores, -jnp.inf), axis=1, keepdims=True))
            exp_scores = jnp.where(visible, jnp.exp(scores - row_max), 0.0)
            denominator = lax.optimization_barrier(jnp.sum(exp_scores, axis=1, keepdims=True))
            weighted = jnp.dot(lifted(exp_scores.astype(jnp.bfloat16)), value_head)
            return weighted / denominator
        head_out = lax.map(one_head, (queries_heads[:, row_low:row_high], qrot_heads[:, row_low:row_high], keys_heads[:, :row_high], values_heads[:, :row_high]))
        pieces.append(jnp.transpose(head_out, (1, 0, 2)).astype(jnp.bfloat16))
    attended = jnp.concatenate(pieces, axis=0).reshape(TOKENS, ATT_WIDTH)
    gated_input = (project(conv_value_weight) * row_scale * jax.nn.sigmoid(project(conv_gate_weight) * row_scale)).astype(jnp.bfloat16)
    padded = jnp.pad(lifted(gated_input), ((KERNEL - 1, 0), (0, 0)))
    conv_out = jnp.zeros((TOKENS, CONV_CH), jnp.float32)
    for tap_idx in range(KERNEL):
        conv_out = conv_out + conv_taps[tap_idx][None, :] * padded[tap_idx:tap_idx + TOKENS]
    mean_val = lax.optimization_barrier(jnp.mean(conv_out, axis=1, keepdims=True))
    spread = lax.optimization_barrier(jnp.mean(conv_out * conv_out, axis=1, keepdims=True)) - mean_val * mean_val
    swished = jax.nn.silu((conv_out - mean_val) * lax.rsqrt(spread + norm_eps) * conv_ln_gain[None, :] + conv_ln_bias[None, :])
    conv_mixed = (swished * lax.rsqrt(lax.optimization_barrier(jnp.mean(swished * swished, axis=1, keepdims=True)) + norm_eps) * conv_out_gain[None, :]).astype(jnp.bfloat16)
    att_wide = lifted(attended)
    att_mixed = (att_wide * lax.rsqrt(lax.optimization_barrier(jnp.mean(att_wide * att_wide, axis=1, keepdims=True)) + norm_eps) * att_out_gain[None, :]).astype(jnp.bfloat16)
    att_share = ATT_WIDTH // N_TP
    conv_share = CONV_CH // N_TP
    result = jnp.zeros((TOKENS, D_MODEL), jnp.float32)
    for group_idx in range(N_TP):
        att_low = group_idx * att_share
        conv_low = group_idx * conv_share
        partial_value = jnp.dot(att_mixed[:, att_low:att_low + att_share].astype(jnp.float32), att_out_weight[att_low:att_low + att_share].astype(jnp.float32), preferred_element_type=jnp.float32) + jnp.dot(conv_mixed[:, conv_low:conv_low + conv_share].astype(jnp.float32), conv_out_weight[conv_low:conv_low + conv_share].astype(jnp.float32), preferred_element_type=jnp.float32)
        result = result + lifted(partial_value.astype(jnp.bfloat16))
    return result.astype(jnp.bfloat16)
```

```python
import functools
import math

import jax
import jax.numpy as jnp
from jax import lax
from jax.experimental import pallas as pl
from jax.experimental.pallas import tpu as pltpu
from jax.sharding import PartitionSpec as P

D_MODEL = 2048
NOPE_DIM = 64
ROT_DIM = 32
VALUE_DIM = 64
CONV_CH = 1024
KERNEL = 31
ATT_WIDTH = 1024

norm_eps = 1e-06
far_below = -1e30
rope_base = 10000.0
SUM_ROWS = 16


def rotary_tables(positions, half_dim):
    frequency = rope_base ** (-jnp.arange(half_dim, dtype=jnp.float32) / half_dim)
    angles = positions.astype(jnp.float32)[:, None] * frequency[None, :]
    return (jnp.cos(angles), jnp.sin(angles))


def rotate_half(values, cos_table, sine_table):
    half_dim = cos_table.shape[-1]
    front_half = values[..., :half_dim]
    back_half = values[..., half_dim:]
    return jnp.concatenate(
        [
            front_half * cos_table - back_half * sine_table,
            back_half * cos_table + front_half * sine_table,
        ],
        axis=-1,
    )


def shift_by(block, axis, distance):
    devices = range(lax.axis_size(axis))
    return lax.ppermute(block, axis, [(i, i + distance) for i in devices if i + distance in devices])


def swap_bits(block, axis, bits):
    return lax.ppermute(block, axis, [(i, i ^ bits) for i in range(lax.axis_size(axis))])


def others(block, axis):
    size = lax.axis_size(axis)
    return [
        lax.ppermute(block, axis, [((i + d) % size, i) for i in range(size)])
        for d in range(1, size)
    ]


def total(block, axis):
    for part in others(block, axis):
        block = block + part
    return block


def in_order(mine, rest, axis, dim):
    size = 1 + len(rest)
    width = mine.shape[dim]
    ring = [mine] + rest + [mine] + rest[:-1]
    start = ((size - lax.axis_index(axis)) % size) * width
    return lax.dynamic_slice_in_dim(jnp.concatenate(ring, axis=dim), start, size * width, dim)


def attention_kernel(first, last, pieces, rows, groups, heads, vis_ref, *refs):
    refs = list(refs)
    qt_ref, qrt_ref, key_up_ref, value_up_ref = refs[:4]
    refs = refs[4:]
    slot_refs, refs = refs[:pieces], refs[pieces:]
    if first:
        (lat_ref, rot_ref), refs = refs[:2], refs[2:]
    else:
        (max_in, acc_in), refs = refs[:2], refs[2:]
    if last:
        (out_ref, max_ref, acc_ref, qbd_ref) = refs
    else:
        (max_ref, acc_ref, qbd_ref) = refs
    step = pl.program_id(0)
    pairs = heads // 2
    queries = qt_ref.shape[1]

    @pl.when(step == 0)
    def start():
        qbd_ref[...] = jnp.zeros_like(qbd_ref)
        for pair in range(pairs):
            for side in range(2):
                head = 2 * pair + side
                columns = slice(side * queries, (side + 1) * queries)
                qbd_ref[pair, side * NOPE_DIM : (side + 1) * NOPE_DIM, columns] = qt_ref[
                    head * NOPE_DIM : (head + 1) * NOPE_DIM, :
                ]
                qbd_ref[pair, 2 * NOPE_DIM : 2 * NOPE_DIM + ROT_DIM, columns] = qrt_ref[
                    head * ROT_DIM : (head + 1) * ROT_DIM, :
                ]
        if first:
            max_ref[...] = jnp.full_like(max_ref, far_below)
            acc_ref[...] = jnp.zeros_like(acc_ref)
        else:
            max_ref[...] = max_in[...]
            acc_ref[...] = acc_in[...]

    def visit(lat, rot, masked):
        count = lat.shape[0]
        keys = jnp.dot(lat, key_up_ref[...], preferred_element_type=jnp.float32).astype(jnp.bfloat16)
        values = lax.dot_general(
            value_up_ref[...], lat, (((1,), (1,)), ((), ())), preferred_element_type=jnp.float32
        ).astype(jnp.bfloat16)
        ones = jnp.ones((SUM_ROWS, count), jnp.bfloat16)
        if masked:
            visible = lax.broadcasted_iota(jnp.int32, (count, queries), 0) <= lax.broadcasted_iota(
                jnp.int32, (count, queries), 1
            )
        for pair in range(pairs):
            key_pair = jnp.concatenate(
                [keys[:, pair * 2 * NOPE_DIM : (pair + 1) * 2 * NOPE_DIM], rot], axis=1
            )
            scores = jnp.dot(key_pair, qbd_ref[pair], preferred_element_type=jnp.float32)
            for side in range(2):
                head = 2 * pair + side
                score = scores[:, side * queries : (side + 1) * queries]
                if masked:
                    score = jnp.where(visible, score, far_below)
                old_max = max_ref[head : head + 1, :]
                new_max = jnp.maximum(old_max, jnp.max(score, axis=0, keepdims=True))
                weights = jnp.exp2(score - new_max).astype(jnp.bfloat16)
                shrink = jnp.exp2(old_max - new_max)
                head_values = jnp.concatenate(
                    [values[head * VALUE_DIM : (head + 1) * VALUE_DIM, :], ones], axis=0
                )
                acc_ref[head] = acc_ref[head] * shrink + jnp.dot(
                    head_values, weights, preferred_element_type=jnp.float32
                )
                max_ref[head : head + 1, :] = new_max

    def from_slots():
        lats, rots = [], []
        for ref in slot_refs:
            lats.append(ref[0, :rows, :])
            packed = ref[0, rows:, :].astype(jnp.float32)[: rows // groups]
            rots += [packed[:, g * ROT_DIM : (g + 1) * ROT_DIM] for g in range(groups)]
        lat = jnp.concatenate(lats, axis=0)
        rot = jnp.concatenate(rots, axis=0)
        rot = jnp.concatenate(
            [rot, jnp.zeros((rot.shape[0], 128 - ROT_DIM), jnp.float32)], axis=1
        ).astype(jnp.bfloat16)
        visit(lat, rot, False)

    if first:

        @pl.when(step == 0)
        def own():
            visit(lat_ref[...], rot_ref[...], True)

        @pl.when((step > 0) & (vis_ref[jnp.maximum(step - 1, 0)] > 0))
        def slot():
            from_slots()

    else:

        @pl.when(vis_ref[step] > 0)
        def slot():
            from_slots()

    if last:

        @pl.when(step == pl.num_programs(0) - 1)
        def finish():
            for pair in range(pairs):
                both = jnp.concatenate(
                    [
                        acc_ref[2 * pair + side, :VALUE_DIM, :]
                        / acc_ref[2 * pair + side, VALUE_DIM : VALUE_DIM + 1, :]
                        for side in range(2)
                    ],
                    axis=0,
                )
                out_ref[:, pair * 2 * VALUE_DIM : (pair + 1) * 2 * VALUE_DIM] = both.T.astype(
                    out_ref.dtype
                )


def attention_stage(visible, queries_t, query_rot_t, key_up, value_up_t, slots, rows, groups,
                    own=None, state=None, last=False):
    first = own is not None
    heads = key_up.shape[1] // NOPE_DIM
    tok_rows = queries_t.shape[1]
    count = slots[0].shape[0]
    whole = lambda a: pl.BlockSpec(a.shape, lambda i, v: (0,) * a.ndim)
    if first:
        slot_map = lambda i, v: (jnp.maximum(i - 1, 0), 0, 0)
        extra = own
    else:
        slot_map = lambda i, v: (i, 0, 0)
        extra = state
    consts = [queries_t, query_rot_t, key_up, value_up_t]
    acc_shape = (heads, VALUE_DIM + SUM_ROWS, tok_rows)
    max_shape = (heads, tok_rows)
    qbd = pltpu.VMEM((heads // 2, 256, 2 * tok_rows), jnp.bfloat16)
    if last:
        out_shape = jax.ShapeDtypeStruct((tok_rows, heads * VALUE_DIM), jnp.bfloat16)
        out_specs = pl.BlockSpec(out_shape.shape, lambda i, v: (0, 0))
        scratch = [pltpu.VMEM(max_shape, jnp.float32), pltpu.VMEM(acc_shape, jnp.float32), qbd]
    else:
        out_shape = (
            jax.ShapeDtypeStruct(max_shape, jnp.float32),
            jax.ShapeDtypeStruct(acc_shape, jnp.float32),
        )
        out_specs = tuple(pl.BlockSpec(s.shape, lambda i, v, n=len(s.shape): (0,) * n) for s in out_shape)
        scratch = [qbd]
    flops = 2 * count * tok_rows * tok_rows * heads * (256 + VALUE_DIM)
    return pl.pallas_call(
        functools.partial(attention_kernel, first, last, len(slots), rows, groups, heads),
        grid_spec=pltpu.PrefetchScalarGridSpec(
            num_scalar_prefetch=1,
            grid=(count + (1 if first else 0),),
            in_specs=[whole(a) for a in consts]
            + [pl.BlockSpec((1,) + s.shape[1:], slot_map) for s in slots]
            + [whole(a) for a in extra],
            out_specs=out_specs,
            scratch_shapes=scratch,
        ),
        out_shape=out_shape,
        compiler_params=pltpu.CompilerParams(
            dimension_semantics=("arbitrary",), vmem_limit_bytes=48 * 1024 * 1024
        ),
        cost_estimate=pl.CostEstimate(
            flops=flops, bytes_accessed=4 << 20, transcendentals=count * tok_rows * tok_rows * heads
        ),
        name="attention_first" if first else "attention_rest",
    )(visible, *consts, *slots, *extra)


def conv_kernel(rim, gated_ref, rim_ref, taps_ref, out_ref, padded_ref):
    rows, chans = gated_ref.shape
    padded_ref[:rim, :] = rim_ref[...].astype(jnp.float32)
    padded_ref[rim : rim + rows, :] = gated_ref[...].astype(jnp.float32)
    offset = rim - (KERNEL - 1)
    step = math.gcd(rows, 64)
    for lane in range(0, chans, 128):
        lanes = slice(lane, lane + 128)
        for row in range(0, rows, step):
            acc = jnp.zeros((step, 128), jnp.float32)
            for phase in range(8):
                taps = range(phase, KERNEL, 8)
                start = row + offset + phase
                part = padded_ref[start : start + step + 8 * (len(taps) - 1), lanes]
                for j, tap in enumerate(taps):
                    acc = acc + taps_ref[tap : tap + 1, lanes] * part[8 * j : 8 * j + step]
            out_ref[row : row + step, lanes] = acc


def convolve(gated, rim, taps):
    rows, chans = gated.shape
    rim_rows = rim.shape[0]
    return pl.pallas_call(
        functools.partial(conv_kernel, rim_rows),
        out_shape=jax.ShapeDtypeStruct((rows, chans), jnp.float32),
        scratch_shapes=[pltpu.VMEM((rim_rows + rows, chans), jnp.float32)],
        cost_estimate=pl.CostEstimate(
            flops=2 * KERNEL * rows * chans * 50, bytes_accessed=6 * rows * chans, transcendentals=0
        ),
        name="conv",
    )(gated, rim, taps)


def shards(
    tokens,
    input_gain,
    query_weight,
    query_rot_weight,
    kv_down,
    rot_down,
    kv_gain,
    key_up,
    value_up,
    conv_value_weight,
    conv_gate_weight,
    conv_taps,
    conv_ln_gain,
    conv_ln_bias,
    att_out_gain,
    conv_out_gain,
    att_out_weight,
    conv_out_weight,
):
    tok_rows = tokens.shape[0]
    heads_here = key_up.shape[1] // NOPE_DIM
    tp_size, sp_size = lax.axis_size("tp"), lax.axis_size("sp")
    tp_index, sp_index = lax.axis_index("tp"), lax.axis_index("sp")
    f32, bf16 = jnp.float32, jnp.bfloat16

    wide = in_order(tokens, others(tokens, "tp"), "tp", 1).astype(f32)
    scaled = (wide * input_gain[None, :]).astype(bf16)
    row_scale = lax.rsqrt(jnp.sum(wide * wide, axis=1) / D_MODEL + norm_eps)[:, None]
    positions = sp_index * tok_rows + jnp.arange(tok_rows, dtype=jnp.int32)
    cos_table, sine_table = rotary_tables(positions, ROT_DIM // 2)

    def project(weight):
        return jnp.dot(scaled, weight, preferred_element_type=f32)

    latent_raw = project(kv_down)
    latent = (
        latent_raw
        * lax.rsqrt(jnp.mean(latent_raw * latent_raw, axis=1, keepdims=True) + norm_eps)
        * kv_gain[None, :]
    ).astype(bf16)
    key_rot = rotate_half(project(rot_down) * row_scale, cos_table, sine_table).astype(bf16)

    rows = tok_rows // tp_size
    rank = latent.shape[1]
    groups = max(
        g for g in range(1, rank // ROT_DIM + 1) if rows % g == 0 and (rows // g) % 8 == 0
    )
    my_lat = lax.dynamic_slice_in_dim(latent, tp_index * rows, rows, 0)
    my_rot = lax.dynamic_slice_in_dim(key_rot, tp_index * rows, rows, 0)
    packed = (
        my_rot.reshape(groups, rows // groups, ROT_DIM)
        .transpose(1, 0, 2)
        .reshape(rows // groups, groups * ROT_DIM)
    )
    packed = jnp.pad(
        packed, ((0, -(rows // groups) % 16), (0, rank - groups * ROT_DIM))
    )
    mine = jnp.concatenate([my_lat, packed], axis=0)

    plane = 4 if sp_size % 4 == 0 else 1
    high, low = sp_index // plane, sp_index % plane
    far = range(1, sp_size // plane)
    near_sent = [swap_bits(mine, "sp", b) for b in range(1, plane)]
    column = [shift_by(mine, "sp", plane * s) for s in far]
    near_vis = [((low ^ b) < low).astype(jnp.int32) for b in range(1, plane)]
    column_vis = [(high >= s).astype(jnp.int32) for s in far]
    slots_one = jnp.stack(near_sent + column)
    vis_one = jnp.stack(near_vis + column_vis)
    slots_one = [slots_one] + others(slots_one, "tp")
    if plane == 4:
        column_all = jnp.stack(column)
        rest = [swap_bits(column_all, "sp", 1), swap_bits(column_all, "sp", 2)]
        rest.append(jnp.stack([shift_by(near_sent[2], "sp", plane * s) for s in far]))
        slots_two = jnp.concatenate(rest, axis=0)
        vis_two = jnp.stack(column_vis * 3)
        slots_two = [slots_two] + others(slots_two, "tp")

    gated = (project(conv_value_weight) * row_scale * jax.nn.sigmoid(project(conv_gate_weight) * row_scale)).astype(bf16)
    rim_rows = 32
    rim = shift_by(gated[tok_rows - rim_rows :], "sp", 1)
    conv_out = convolve(gated, rim, conv_taps)
    moments = total(jnp.stack([jnp.sum(conv_out, axis=1), jnp.sum(conv_out * conv_out, axis=1)]), "tp")
    mean_val = moments[0] / CONV_CH
    spread = moments[1] / CONV_CH - mean_val * mean_val
    normed = (conv_out - mean_val[:, None]) * lax.rsqrt(spread + norm_eps)[:, None]
    swished = jax.nn.silu(normed * conv_ln_gain[None, :] + conv_ln_bias[None, :])
    conv_sq = total(jnp.sum(swished * swished, axis=1)[None, :], "tp")[0]
    conv_mixed = (
        swished * lax.rsqrt(conv_sq / CONV_CH + norm_eps)[:, None] * conv_out_gain[None, :]
    ).astype(bf16)
    conv_part = jnp.dot(conv_mixed, conv_out_weight, preferred_element_type=f32)

    query_scale = row_scale * (math.log2(math.e) / math.sqrt(NOPE_DIM + ROT_DIM))
    queries_t = (project(query_weight) * query_scale).astype(bf16).T
    query_rot_t = (
        rotate_half(
            (project(query_rot_weight) * query_scale).reshape(tok_rows, heads_here, ROT_DIM),
            cos_table[:, None, :],
            sine_table[:, None, :],
        )
        .astype(bf16)
        .reshape(tok_rows, heads_here * ROT_DIM)
        .T
    )
    value_up_t = value_up.T
    own = (latent, jnp.pad(key_rot, ((0, 0), (0, 128 - ROT_DIM))))
    stage = functools.partial(
        attention_stage,
        queries_t=queries_t,
        query_rot_t=query_rot_t,
        key_up=key_up,
        value_up_t=value_up_t,
        rows=rows,
        groups=groups,
    )
    if plane == 4:
        state = stage(vis_one, slots=slots_one, own=own)
        attended = stage(vis_two, slots=slots_two, state=state, last=True)
    else:
        attended = stage(vis_one, slots=slots_one, own=own, last=True)

    attended = attended.astype(f32)
    att_sq = total(jnp.sum(attended * attended, axis=1)[None, :], "tp")[0]
    att_part = jnp.dot(
        (attended * att_out_gain[None, :]).astype(bf16), att_out_weight, preferred_element_type=f32
    )
    partial = (att_part * lax.rsqrt(att_sq / ATT_WIDTH + norm_eps)[:, None] + conv_part).astype(bf16)
    width = D_MODEL // tp_size
    mixed = lax.dynamic_slice_in_dim(partial, tp_index * width, width, 1).astype(f32)
    for d in range(1, tp_size):
        target = (tp_index + tp_size - d) % tp_size
        send = lax.dynamic_slice_in_dim(partial, target * width, width, 1)
        mixed = mixed + lax.ppermute(
            send, "tp", [((i + d) % tp_size, i) for i in range(tp_size)]
        ).astype(f32)
    return mixed.astype(bf16)


def solution(mesh):
    return jax.shard_map(
        shards,
        mesh=mesh,
        in_specs=(
            P("sp", "tp"),
            P(),
            P(None, "tp"),
            P(None, "tp"),
            P(),
            P(),
            P(),
            P(None, "tp"),
            P(None, "tp"),
            P(None, "tp"),
            P(None, "tp"),
            P(None, "tp"),
            P("tp"),
            P("tp"),
            P("tp"),
            P("tp"),
            P("tp", None),
            P("tp", None),
        ),
        out_specs=P("sp", "tp"),
        check_vma=False,
    )
```

```python
import functools
import math

import jax
import jax.numpy as jnp
from jax import lax
from jax.experimental import pallas as pl
from jax.experimental.pallas import tpu as pltpu
from jax.sharding import PartitionSpec as P

D_MODEL = 2048
NOPE_DIM = 64
ROT_DIM = 32
VALUE_DIM = 64
CONV_CH = 1024
KERNEL = 31
ATT_WIDTH = 1024


norm_eps = 1e-06
far_below = -1e30
rope_base = 10000.0
SUM_ROWS = 16


def rotary_tables(positions, half_dim):
    frequency = rope_base ** (-jnp.arange(half_dim, dtype=jnp.float32) / half_dim)
    angles = positions.astype(jnp.float32)[:, None] * frequency[None, :]
    return (jnp.cos(angles), jnp.sin(angles))


def rotate_half(values, cos_table, sine_table):
    half_dim = cos_table.shape[-1]
    front_half = values[..., :half_dim]
    back_half = values[..., half_dim:]
    return jnp.concatenate(
        [
            front_half * cos_table - back_half * sine_table,
            back_half * cos_table + front_half * sine_table,
        ],
        axis=-1,
    )


def shift_by(block, axis, distance):
    devices = range(lax.axis_size(axis))
    return lax.ppermute(block, axis, [(i, i + distance) for i in devices if i + distance in devices])


def swap_bits(block, axis, bits):
    return lax.ppermute(block, axis, [(i, i ^ bits) for i in range(lax.axis_size(axis))])


def others(block, axis):
    size = lax.axis_size(axis)
    return [
        lax.ppermute(block, axis, [((i + d) % size, i) for i in range(size)])
        for d in range(1, size)
    ]


def total(block, axis):
    for part in others(block, axis):
        block = block + part
    return block


def in_order(mine, rest, axis, dim):
    size = 1 + len(rest)
    width = mine.shape[dim]
    ring = [mine] + rest + [mine] + rest[:-1]
    start = ((size - lax.axis_index(axis)) % size) * width
    return lax.dynamic_slice_in_dim(jnp.concatenate(ring, axis=dim), start, size * width, dim)


def tiles_of(queries):
    width = 256 if (2 * queries) % 256 == 0 else queries
    out = []
    for start in range(0, 2 * queries, width):
        parts = []
        for side in range(2):
            low = max(start, side * queries)
            high = min(start + width, (side + 1) * queries)
            if low < high:
                parts.append((side, low - start, high - start))
        out.append((start, parts))
    return width, out


def attention_kernel(first, last, counts, rows, groups, heads, vis_ref, *refs):
    refs = list(refs)
    qt_ref, qrt_ref, key_up_ref, value_up_ref = refs[:4]
    refs = refs[4:]
    pieces = len(counts[0])
    sources = []
    for _ in counts:
        sources.append(refs[:pieces])
        refs = refs[pieces:]
    if first:
        (own_lat_ref, own_rot_ref), refs = refs[:2], refs[2:]
    else:
        (max_in, acc_in), refs = refs[:2], refs[2:]
    if last:
        (out_ref, max_ref, acc_ref), refs = refs[:3], refs[3:]
    else:
        (max_ref, acc_ref), refs = refs[:2], refs[2:]
    lat_ref, rot_ref, qbd_ref, score_refs, weight_refs, refs = (
        refs[0], refs[1], refs[2], refs[3:5], refs[5:7], refs[7:]
    )
    pairs = heads // 2
    parcels = max(1, pairs // 2)
    key_refs, values_refs = refs[:parcels], refs[parcels:]
    per = pairs // parcels
    queries = qt_ref.shape[1]
    width, tiles = tiles_of(queries)
    head_rows = VALUE_DIM + SUM_ROWS
    blocks = lat_ref.shape[0]
    bias_row = 2 * NOPE_DIM + ROT_DIM

    qbd_ref[...] = jnp.zeros_like(qbd_ref)
    for pair in range(pairs):
        qbd_ref[pair, bias_row : bias_row + 16, :] = (
            lax.broadcasted_iota(jnp.int32, (16, 2 * queries), 0) == 0
        ).astype(jnp.bfloat16)
        for side in range(2):
            head = 2 * pair + side
            columns = slice(side * queries, (side + 1) * queries)
            qbd_ref[pair, side * NOPE_DIM : (side + 1) * NOPE_DIM, columns] = qt_ref[
                head * NOPE_DIM : (head + 1) * NOPE_DIM, :
            ]
            qbd_ref[pair, 2 * NOPE_DIM : 2 * NOPE_DIM + ROT_DIM, columns] = qrt_ref[
                head * ROT_DIM : (head + 1) * ROT_DIM, :
            ]
    for ref in values_refs:
        ref[...] = jnp.ones_like(ref)
    if first:
        max_ref[...] = jnp.full_like(max_ref, far_below)
        acc_ref[...] = jnp.zeros_like(acc_ref)
        lat_ref[0, :queries, :] = own_lat_ref[...]
        rot_ref[0, :queries, :] = own_rot_ref[...]
    else:
        max_ref[...] = max_in[...]
        acc_ref[...] = acc_in[...]

    at = 1 if first else 0
    slot = 0
    is_bias = lax.broadcasted_iota(jnp.int32, (queries, 128), 1) == ROT_DIM
    for source, several in zip(sources, counts):
        for index in range(several[0] or 1):
            rots = []
            base = (at % 2) * queries
            for n, ref in enumerate(source):
                view = ref.at[index] if several[0] else ref
                lat_ref[at // 2, base + n * rows : base + (n + 1) * rows, :] = view[:rows, :]
                packed = view[rows:, :].astype(jnp.float32)[: rows // groups]
                rots += [packed[:, g * ROT_DIM : (g + 1) * ROT_DIM] for g in range(groups)]
            rot = jnp.concatenate(rots, axis=0)
            rot = jnp.concatenate([rot, jnp.zeros((queries, 128 - ROT_DIM), jnp.float32)], axis=1)
            bias = jnp.where(vis_ref[slot] > 0, 0.0, far_below)
            rot_ref[at // 2, base : base + queries, :] = jnp.where(is_bias, bias, rot).astype(jnp.bfloat16)
            at += 1
            slot += 1
    if at % 2:
        lat_ref[at // 2, queries:, :] = jnp.zeros((queries, lat_ref.shape[2]), jnp.bfloat16)
        rot_ref[at // 2, queries:, :] = jnp.where(is_bias, far_below, 0.0).astype(jnp.bfloat16)

    def visit(block, masked):
        span = per * 2 * NOPE_DIM
        work = [(pair, i) for pair in range(pairs) for i in range(len(tiles))]
        shrinks = {}

        def expand_keys(n):
            key_refs[n][...] = jnp.dot(
                lat_ref[block],
                key_up_ref[:, n * span : (n + 1) * span],
                preferred_element_type=jnp.float32,
            ).astype(jnp.bfloat16)

        def expand_values(n):
            values = lax.dot_general(
                value_up_ref[n * span : (n + 1) * span, :],
                lat_ref[block],
                (((1,), (1,)), ((), ())),
                preferred_element_type=jnp.float32,
            ).astype(jnp.bfloat16)
            for head in range(2 * per):
                values_refs[n][head * head_rows : head * head_rows + VALUE_DIM, :] = values[
                    head * VALUE_DIM : (head + 1) * VALUE_DIM, :
                ]

        def product(at):
            pair, i = work[at]
            begin = tiles[i][0]
            within = (pair % per) * 2 * NOPE_DIM
            key_pair = jnp.concatenate(
                [key_refs[pair // per][:, within : within + 2 * NOPE_DIM], rot_ref[block]], axis=1
            )
            score = jnp.dot(
                key_pair, qbd_ref[pair, :, begin : begin + width], preferred_element_type=jnp.float32
            )
            if masked:
                column = lax.broadcasted_iota(jnp.int32, (queries, width), 1) + begin
                column = jnp.where(column >= queries, column - queries, column)
                visible = lax.broadcasted_iota(jnp.int32, (queries, width), 0) <= column
                score_refs[at % 2][:queries, :] = jnp.where(visible, score[:queries], far_below)
                score_refs[at % 2][queries:, :] = score[queries:]
            else:
                score_refs[at % 2][...] = score

        def soften(at):
            old_max = max_ref[at : at + 1, :]
            score = score_refs[at % 2]
            new_max = jnp.maximum(old_max, jnp.max(score[...], axis=0, keepdims=True))
            weight_refs[at % 2][...] = jnp.exp2(score[...] - new_max).astype(jnp.bfloat16)
            shrinks[at] = jnp.exp2(old_max - new_max)
            max_ref[at : at + 1, :] = new_max

        def weigh(at):
            pair, i = work[at]
            parts = tiles[i][1]
            head = 2 * (pair % per) + parts[0][0]
            fresh = jnp.dot(
                values_refs[pair // per][head * head_rows : (head + len(parts)) * head_rows, :],
                weight_refs[at % 2][...],
                preferred_element_type=jnp.float32,
            )
            if len(parts) > 1:
                fresh = jnp.concatenate(
                    [
                        fresh[n * head_rows : (n + 1) * head_rows, low:high]
                        for n, (_, low, high) in enumerate(parts)
                    ],
                    axis=1,
                )
            acc_ref[at] = acc_ref[at] * shrinks[at] + fresh

        share = per * len(tiles)
        expand_keys(0)
        product(0)
        expand_values(0)
        for at in range(len(work) + 1):
            ahead = (at + 3) // share
            if (at + 3) % share == 0 and 0 < ahead < parcels:
                expand_keys(ahead)
            ahead = (at + 1) // share
            if (at + 1) % share == 0 and 0 < ahead < parcels:
                expand_values(ahead)
            if at + 1 < len(work):
                product(at + 1)
            if at < len(work):
                soften(at)
            if at > 0:
                weigh(at - 1)

    if first:
        visit(0, True)

    @pl.loop(1 if first else 0, blocks)
    def each_block(block):
        low = 2 * block - (1 if first else 0)
        high = jnp.minimum(low + 1, slot - 1)

        @pl.when((vis_ref[low] > 0) | (vis_ref[high] > 0))
        def seen():
            visit(block, False)

    if last:
        for pair in range(pairs):
            pieces_of = ([], [])
            for i, (_, parts) in enumerate(tiles):
                done = acc_ref[pair * len(tiles) + i]
                done = done[:VALUE_DIM] / done[VALUE_DIM : VALUE_DIM + 1]
                for side, low, high in parts:
                    pieces_of[side].append(done[:, low:high])
            both = jnp.concatenate([jnp.concatenate(p, axis=1) for p in pieces_of], axis=0)
            out_ref[:, pair * 2 * VALUE_DIM : (pair + 1) * 2 * VALUE_DIM] = both.T.astype(out_ref.dtype)


def attention_stage(visible, queries_t, query_rot_t, key_up, value_up_t, slots, rows, groups,
                    own=None, state=None, last=False):
    first = own is not None
    heads = key_up.shape[1] // NOPE_DIM
    tok_rows = queries_t.shape[1]
    counts = [[p.shape[0] if p.ndim == 3 else 0 for p in s] for s in slots]
    total_blocks = sum(c[0] or 1 for c in counts) + (1 if first else 0)
    blocks = (total_blocks + 1) // 2
    width, tiles = tiles_of(tok_rows)
    tile_count = heads // 2 * len(tiles)
    extra = own if first else state
    consts = [queries_t, query_rot_t, key_up, value_up_t]
    flat = [p for s in slots for p in s]
    acc_shape = (tile_count, VALUE_DIM + SUM_ROWS, width)
    max_shape = (tile_count, width)
    parcels = max(1, heads // 4)
    keys = 2 * tok_rows
    scratch = (
        [
            pltpu.VMEM((blocks, keys, key_up.shape[0]), jnp.bfloat16),
            pltpu.VMEM((blocks, keys, 128), jnp.bfloat16),
            pltpu.VMEM((heads // 2, 256, 2 * tok_rows), jnp.bfloat16),
        ]
        + [pltpu.VMEM((keys, width), jnp.float32)] * 2
        + [pltpu.VMEM((keys, width), jnp.bfloat16)] * 2
        + [pltpu.VMEM((keys, heads // parcels * NOPE_DIM), jnp.bfloat16)] * parcels
        + [pltpu.VMEM((heads // parcels * (VALUE_DIM + SUM_ROWS), keys), jnp.bfloat16)] * parcels
    )
    if last:
        out_shape = jax.ShapeDtypeStruct((tok_rows, heads * VALUE_DIM), jnp.bfloat16)
        scratch = [pltpu.VMEM(max_shape, jnp.float32), pltpu.VMEM(acc_shape, jnp.float32)] + scratch
    else:
        out_shape = (
            jax.ShapeDtypeStruct(max_shape, jnp.float32),
            jax.ShapeDtypeStruct(acc_shape, jnp.float32),
        )
    flops = 2 * total_blocks * tok_rows * tok_rows * heads * (256 + VALUE_DIM)
    in_vmem = pl.BlockSpec(memory_space=pltpu.VMEM)
    return pl.pallas_call(
        functools.partial(attention_kernel, first, last, counts, rows, groups, heads),
        in_specs=[pl.BlockSpec(memory_space=pltpu.SMEM)] + [in_vmem] * (len(consts) + len(flat) + len(extra)),
        out_specs=in_vmem if last else (in_vmem, in_vmem),
        scratch_shapes=scratch,
        out_shape=out_shape,
        compiler_params=pltpu.CompilerParams(vmem_limit_bytes=24 * 1024 * 1024),
        cost_estimate=pl.CostEstimate(
            flops=flops, bytes_accessed=4 << 20, transcendentals=total_blocks * tok_rows * tok_rows * heads
        ),
        name="attention_first" if first else "attention_rest",
    )(visible, *consts, *flat, *extra)


def conv_kernel(rim, gated_ref, rim_ref, taps_ref, out_ref, padded_ref):
    rows, chans = gated_ref.shape
    padded_ref[:rim, :] = rim_ref[...].astype(jnp.float32)
    padded_ref[rim : rim + rows, :] = gated_ref[...].astype(jnp.float32)
    offset = rim - (KERNEL - 1)
    step = math.gcd(rows, 64)
    for lane in range(0, chans, 128):
        lanes = slice(lane, lane + 128)
        for row in range(0, rows, step):
            acc = jnp.zeros((step, 128), jnp.float32)
            for phase in range(8):
                taps = range(phase, KERNEL, 8)
                start = row + offset + phase
                part = padded_ref[start : start + step + 8 * (len(taps) - 1), lanes]
                for j, tap in enumerate(taps):
                    acc = acc + taps_ref[tap : tap + 1, lanes] * part[8 * j : 8 * j + step]
            out_ref[row : row + step, lanes] = acc


def convolve(gated, rim, taps):
    rows, chans = gated.shape
    rim_rows = rim.shape[0]
    return pl.pallas_call(
        functools.partial(conv_kernel, rim_rows),
        out_shape=jax.ShapeDtypeStruct((rows, chans), jnp.float32),
        scratch_shapes=[pltpu.VMEM((rim_rows + rows, chans), jnp.float32)],
        cost_estimate=pl.CostEstimate(
            flops=2 * KERNEL * rows * chans * 50, bytes_accessed=6 * rows * chans, transcendentals=0
        ),
        name="conv",
    )(gated, rim, taps)


def shards(
    tokens,
    input_gain,
    query_weight,
    query_rot_weight,
    kv_down,
    rot_down,
    kv_gain,
    key_up,
    value_up,
    conv_value_weight,
    conv_gate_weight,
    conv_taps,
    conv_ln_gain,
    conv_ln_bias,
    att_out_gain,
    conv_out_gain,
    att_out_weight,
    conv_out_weight,
):
    tok_rows = tokens.shape[0]
    heads_here = key_up.shape[1] // NOPE_DIM
    tp_size, sp_size = lax.axis_size("tp"), lax.axis_size("sp")
    tp_index, sp_index = lax.axis_index("tp"), lax.axis_index("sp")
    f32, bf16 = jnp.float32, jnp.bfloat16

    wide = in_order(tokens, others(tokens, "tp"), "tp", 1).astype(f32)
    scaled = (wide * input_gain[None, :]).astype(bf16)
    row_scale = lax.rsqrt(jnp.sum(wide * wide, axis=1) / D_MODEL + norm_eps)[:, None]
    positions = sp_index * tok_rows + jnp.arange(tok_rows, dtype=jnp.int32)
    cos_table, sine_table = rotary_tables(positions, ROT_DIM // 2)

    def project(weight):
        return jnp.dot(scaled, weight, preferred_element_type=f32)

    latent_raw = project(kv_down)
    latent = (
        latent_raw
        * lax.rsqrt(jnp.mean(latent_raw * latent_raw, axis=1, keepdims=True) + norm_eps)
        * kv_gain[None, :]
    ).astype(bf16)
    key_rot = rotate_half(project(rot_down) * row_scale, cos_table, sine_table).astype(bf16)

    rows = tok_rows // tp_size
    rank = latent.shape[1]
    groups = max(
        g for g in range(1, rank // ROT_DIM + 1) if rows % g == 0 and (rows // g) % 8 == 0
    )
    my_lat = lax.dynamic_slice_in_dim(latent, tp_index * rows, rows, 0)
    my_rot = lax.dynamic_slice_in_dim(key_rot, tp_index * rows, rows, 0)
    packed = (
        my_rot.reshape(groups, rows // groups, ROT_DIM)
        .transpose(1, 0, 2)
        .reshape(rows // groups, groups * ROT_DIM)
    )
    packed = jnp.pad(
        packed, ((0, -(rows // groups) % 16), (0, rank - groups * ROT_DIM))
    )
    mine = jnp.concatenate([my_lat, packed], axis=0)

    plane = 4 if sp_size % 4 == 0 else 1
    high, low = sp_index // plane, sp_index % plane
    far = range(1, sp_size // plane)
    near = [swap_bits(mine, "sp", b) for b in range(1, plane)]
    column = [shift_by(mine, "sp", plane * s) for s in far]
    near_vis = [((low ^ b) < low).astype(jnp.int32) for b in range(1, plane)]
    column_vis = [(high >= s).astype(jnp.int32) for s in far]

    def with_pieces(arrays):
        return [[a] + others(a, "tp") for a in arrays]

    slots_one, vis_one = with_pieces(near + column), near_vis + column_vis
    slots_two, vis_two = [], []
    if plane == 4:
        if len(slots_one) % 2 == 0:
            slots_two, vis_two = slots_one[-1:], vis_one[-1:]
            slots_one, vis_one = slots_one[:-1], vis_one[:-1]
        column_all = jnp.stack(column)
        across = [swap_bits(column_all, "sp", 1), swap_bits(column_all, "sp", 2)]
        diagonal = [shift_by(near[2], "sp", plane * s) for s in far]
        slots_two = slots_two + with_pieces(across + diagonal)
        vis_two = vis_two + column_vis * 3

    gated = (project(conv_value_weight) * row_scale * jax.nn.sigmoid(project(conv_gate_weight) * row_scale)).astype(bf16)
    rim_rows = 32
    rim = shift_by(gated[tok_rows - rim_rows :], "sp", 1)
    conv_out = convolve(gated, rim, conv_taps)
    moments = total(jnp.stack([jnp.sum(conv_out, axis=1), jnp.sum(conv_out * conv_out, axis=1)]), "tp")
    mean_val = moments[0] / CONV_CH
    spread = moments[1] / CONV_CH - mean_val * mean_val
    normed = (conv_out - mean_val[:, None]) * lax.rsqrt(spread + norm_eps)[:, None]
    swished = jax.nn.silu(normed * conv_ln_gain[None, :] + conv_ln_bias[None, :])
    conv_sq = total(jnp.sum(swished * swished, axis=1)[None, :], "tp")[0]
    conv_mixed = (
        swished * lax.rsqrt(conv_sq / CONV_CH + norm_eps)[:, None] * conv_out_gain[None, :]
    ).astype(bf16)
    width = D_MODEL // tp_size

    def columns_of(device, weight):
        return lax.dynamic_slice_in_dim(weight, device * width, width, 1)

    def scatter(product):
        parts = []
        for d in range(1, tp_size):
            send = product((tp_index + tp_size - d) % tp_size).astype(bf16)
            parts.append(
                lax.ppermute(send, "tp", [((i + d) % tp_size, i) for i in range(tp_size)])
            )
        result = product(tp_index)
        for part in parts:
            result = result + part.astype(f32)
        return result

    conv_part = scatter(
        lambda device: jnp.dot(
            conv_mixed, columns_of(device, conv_out_weight), preferred_element_type=f32
        )
    )

    query_scale = row_scale * (math.log2(math.e) / math.sqrt(NOPE_DIM + ROT_DIM))
    queries_t = (project(query_weight) * query_scale).astype(bf16).T
    query_rot_t = (
        rotate_half(
            (project(query_rot_weight) * query_scale).reshape(tok_rows, heads_here, ROT_DIM),
            cos_table[:, None, :],
            sine_table[:, None, :],
        )
        .astype(bf16)
        .reshape(tok_rows, heads_here * ROT_DIM)
        .T
    )
    value_up_t = value_up.T
    own = (latent, jnp.pad(key_rot, ((0, 0), (0, 128 - ROT_DIM))))
    stage = functools.partial(
        attention_stage,
        queries_t=queries_t,
        query_rot_t=query_rot_t,
        key_up=key_up,
        value_up_t=value_up_t,
        rows=rows,
        groups=groups,
    )
    if slots_two:
        state = stage(jnp.stack(vis_one), slots=slots_one, own=own)
        attended = stage(jnp.stack(vis_two), slots=slots_two, state=state, last=True)
    else:
        attended = stage(jnp.stack(vis_one), slots=slots_one, own=own, last=True)

    wide_att = attended.astype(f32)
    att_sq = total(jnp.sum(wide_att * wide_att, axis=1)[None, :], "tp")[0]
    gained = (wide_att * att_out_gain[None, :]).astype(bf16)
    att_part = scatter(
        lambda device: jnp.dot(gained, columns_of(device, att_out_weight), preferred_element_type=f32)
    )
    return (att_part * lax.rsqrt(att_sq / ATT_WIDTH + norm_eps)[:, None] + conv_part).astype(bf16)


def solution(mesh):
    return jax.shard_map(
        shards,
        mesh=mesh,
        in_specs=(
            P("sp", "tp"),
            P(),
            P(None, "tp"),
            P(None, "tp"),
            P(),
            P(),
            P(),
            P(None, "tp"),
            P(None, "tp"),
            P(None, "tp"),
            P(None, "tp"),
            P(None, "tp"),
            P("tp"),
            P("tp"),
            P("tp"),
            P("tp"),
            P("tp", None),
            P("tp", None),
        ),
        out_specs=P("sp", "tp"),
        check_vma=False,
    )
```

```python
import functools
import math

import jax
import jax.numpy as jnp
from jax import lax
from jax.experimental import pallas as pl
from jax.experimental.pallas import tpu as pltpu
from jax.sharding import PartitionSpec as P


D_MODEL = 2048
NOPE_DIM = 64
ROT_DIM = 32
VALUE_DIM = 64
CONV_CH = 1024
KERNEL = 31
ATT_WIDTH = 1024


norm_eps = 1e-06
far_below = -1e30
rope_base = 10000.0
SUM_ROWS = 16


def rotary_tables(positions, half_dim):
    frequency = rope_base ** (-jnp.arange(half_dim, dtype=jnp.float32) / half_dim)
    angles = positions.astype(jnp.float32)[:, None] * frequency[None, :]
    return (jnp.cos(angles), jnp.sin(angles))


def rotate_half(values, cos_table, sine_table):
    half_dim = cos_table.shape[-1]
    front_half = values[..., :half_dim]
    back_half = values[..., half_dim:]
    return jnp.concatenate(
        [
            front_half * cos_table - back_half * sine_table,
            back_half * cos_table + front_half * sine_table,
        ],
        axis=-1,
    )


def shift_by(block, axis, distance):
    devices = range(lax.axis_size(axis))
    return lax.ppermute(block, axis, [(i, i + distance) for i in devices if i + distance in devices])


def swap_bits(block, axis, bits):
    return lax.ppermute(block, axis, [(i, i ^ bits) for i in range(lax.axis_size(axis))])


def others(block, axis):
    size = lax.axis_size(axis)
    return [
        lax.ppermute(block, axis, [((i + d) % size, i) for i in range(size)])
        for d in range(1, size)
    ]


def total(block, axis):
    for part in others(block, axis):
        block = block + part
    return block


def front_kernel(pieces, rows, groups, index_ref, *refs):
    token_refs, refs = refs[:pieces], refs[pieces:]
    gain_ref, down_ref, rot_down_ref, kv_gain_ref, cos_ref, sin_ref = refs[:6]
    scaled_ref, scale_ref, lat_ref, rot_ref, send_ref, wide_rot_ref = refs[6:]
    me = index_ref[0]
    tok_rows, width = token_refs[0].shape
    squares = jnp.zeros((tok_rows, 128), jnp.float32)
    for d, ref in enumerate(token_refs):
        begin = lax.rem(me + d, pieces) * width
        for col in range(0, width, 128):
            at = pl.ds(pl.multiple_of(begin + col, 128), 128)
            values = ref[:, col : col + 128].astype(jnp.float32)
            scaled_ref[:, at] = (values * gain_ref[:, at]).astype(jnp.bfloat16)
            squares = squares + values * values
    row_scale = lax.rsqrt(jnp.sum(squares, axis=1, keepdims=True) / D_MODEL + norm_eps)
    scale_ref[...] = row_scale
    raw = jnp.dot(scaled_ref[...], down_ref[...], preferred_element_type=jnp.float32)
    half = ROT_DIM // 2
    turned = jnp.concatenate(
        [rot_down_ref[...], rot_down_ref[half:, :], rot_down_ref[:half, :]], axis=0
    )
    both = (
        lax.dot_general(
            scaled_ref[...], turned, (((1,), (1,)), ((), ())), preferred_element_type=jnp.float32
        )
        * row_scale
    )
    mean = jnp.mean(raw * raw, axis=1, keepdims=True)
    lat_ref[...] = (raw * lax.rsqrt(mean + norm_eps) * kv_gain_ref[...]).astype(jnp.bfloat16)
    rot = both[:, :ROT_DIM] * cos_ref[...] + both[:, ROT_DIM : 2 * ROT_DIM] * sin_ref[...]
    rot = jnp.concatenate([rot, jnp.zeros((tok_rows, 128 - ROT_DIM), jnp.float32)], axis=1)
    wide_rot_ref[...] = rot
    rot_ref[...] = rot.astype(jnp.bfloat16)
    start = me * rows
    send_ref[:rows, :] = lat_ref[pl.ds(pl.multiple_of(start, 16), rows), :]
    height = rows // groups
    packed = [
        wide_rot_ref[pl.ds(pl.multiple_of(start + g * height, 8), height), :][:, :ROT_DIM]
        for g in range(groups)
    ]
    rank = lat_ref.shape[1]
    if groups * ROT_DIM < rank:
        packed.append(jnp.zeros((height, rank - groups * ROT_DIM), jnp.float32))
    packed = jnp.concatenate(packed, axis=1)
    spare = send_ref.shape[0] - rows - height
    if spare:
        packed = jnp.concatenate([packed, jnp.zeros((spare, rank), jnp.float32)], axis=0)
    send_ref[rows:, :] = packed.astype(jnp.bfloat16)


def front(index, pieces, gain, down, rot_down, kv_gain, cos, sin, groups):
    tok_rows, width = pieces[0].shape
    rank = down.shape[1]
    rows = tok_rows // len(pieces)
    height = rows // groups
    model = width * len(pieces)
    in_vmem = pl.BlockSpec()
    args = list(pieces) + [gain, down, rot_down, kv_gain, cos, sin]
    return pl.pallas_call(
        functools.partial(front_kernel, len(pieces), rows, groups),
        in_specs=[pl.BlockSpec(memory_space=pltpu.SMEM)] + [in_vmem] * len(args),
        out_specs=(in_vmem,) * 5,
        out_shape=(
            jax.ShapeDtypeStruct((tok_rows, model), jnp.bfloat16),
            jax.ShapeDtypeStruct((tok_rows, 1), jnp.float32),
            jax.ShapeDtypeStruct((tok_rows, rank), jnp.bfloat16),
            jax.ShapeDtypeStruct((tok_rows, 128), jnp.bfloat16),
            jax.ShapeDtypeStruct((rows + height + -height % 16, rank), jnp.bfloat16),
        ),
        scratch_shapes=[pltpu.VMEM((tok_rows, 128), jnp.float32)],
        compiler_params=pltpu.CompilerParams(vmem_limit_bytes=16 * 1024 * 1024),
        cost_estimate=pl.CostEstimate(
            flops=2 * tok_rows * model * 512, bytes_accessed=8 << 20, transcendentals=tok_rows
        ),
        name="front",
    )(index, *args)


def tiles_of(queries):
    width = 256 if (2 * queries) % 256 == 0 else queries
    out = []
    for start in range(0, 2 * queries, width):
        parts = []
        for side in range(2):
            low = max(start, side * queries)
            high = min(start + width, (side + 1) * queries)
            if low < high:
                parts.append((side, low - start, high - start))
        out.append((start, parts))
    return width, out


def attention_kernel(first, last, counts, rows, groups, heads, vis_ref, *refs):
    refs = list(refs)
    qt_ref, qrt_ref, key_up_ref, value_up_ref = refs[:4]
    refs = refs[4:]
    pieces = len(counts[0])
    sources = []
    for _ in counts:
        sources.append(refs[:pieces])
        refs = refs[pieces:]
    if first:
        (own_lat_ref, own_rot_ref), refs = refs[:2], refs[2:]
    else:
        (max_in, acc_in), refs = refs[:2], refs[2:]
    if last:
        (out_ref, max_ref, acc_ref), refs = refs[:3], refs[3:]
    else:
        (max_ref, acc_ref), refs = refs[:2], refs[2:]
    lat_ref, rot_ref, qbd_ref, turned_ref, score_refs, weight_refs, refs = (
        refs[0], refs[1], refs[2], refs[3], refs[4:6], refs[6:8], refs[8:]
    )
    pairs = heads // 2
    parcels = max(1, pairs // 2)
    key_refs, values_refs = refs[:parcels], refs[parcels:]
    per = pairs // parcels
    queries = qt_ref.shape[1]
    width, tiles = tiles_of(queries)
    head_rows = VALUE_DIM + SUM_ROWS
    blocks = lat_ref.shape[0]
    bias_row = 2 * NOPE_DIM + ROT_DIM

    turned_ref[...] = value_up_ref[...].T
    qbd_ref[...] = jnp.zeros_like(qbd_ref)
    for pair in range(pairs):
        qbd_ref[pair, bias_row : bias_row + 16, :] = (
            lax.broadcasted_iota(jnp.int32, (16, 2 * queries), 0) == 0
        ).astype(jnp.bfloat16)
        for side in range(2):
            head = 2 * pair + side
            columns = slice(side * queries, (side + 1) * queries)
            qbd_ref[pair, side * NOPE_DIM : (side + 1) * NOPE_DIM, columns] = qt_ref[
                head * NOPE_DIM : (head + 1) * NOPE_DIM, :
            ]
            qbd_ref[pair, 2 * NOPE_DIM : 2 * NOPE_DIM + ROT_DIM, columns] = qrt_ref[
                head * ROT_DIM : (head + 1) * ROT_DIM, :
            ]
    for ref in values_refs:
        ref[...] = jnp.ones_like(ref)
    if first:
        max_ref[...] = jnp.full_like(max_ref, far_below)
        acc_ref[...] = jnp.zeros_like(acc_ref)
        lat_ref[0, :queries, :] = own_lat_ref[...]
        rot_ref[0, :queries, :] = own_rot_ref[...]
    else:
        max_ref[...] = max_in[...]
        acc_ref[...] = acc_in[...]

    at = 1 if first else 0
    slot = 0
    is_bias = lax.broadcasted_iota(jnp.int32, (queries, 128), 1) == ROT_DIM
    for source, several in zip(sources, counts):
        for index in range(several[0] or 1):
            rots = []
            base = (at % 2) * queries
            for n, ref in enumerate(source):
                view = ref.at[index] if several[0] else ref
                lat_ref[at // 2, base + n * rows : base + (n + 1) * rows, :] = view[:rows, :]
                packed = view[rows:, :].astype(jnp.float32)[: rows // groups]
                rots += [packed[:, g * ROT_DIM : (g + 1) * ROT_DIM] for g in range(groups)]
            rot = jnp.concatenate(rots, axis=0)
            rot = jnp.concatenate([rot, jnp.zeros((queries, 128 - ROT_DIM), jnp.float32)], axis=1)
            bias = jnp.where(vis_ref[slot] > 0, 0.0, far_below)
            rot_ref[at // 2, base : base + queries, :] = jnp.where(is_bias, bias, rot).astype(jnp.bfloat16)
            at += 1
            slot += 1
    if at % 2:
        lat_ref[at // 2, queries:, :] = jnp.zeros((queries, lat_ref.shape[2]), jnp.bfloat16)
        rot_ref[at // 2, queries:, :] = jnp.where(is_bias, far_below, 0.0).astype(jnp.bfloat16)

    def visit(block, masked):
        span = per * 2 * NOPE_DIM
        work = [(pair, i) for pair in range(pairs) for i in range(len(tiles))]
        shrinks = {}

        def expand_keys(n):
            key_refs[n][...] = jnp.dot(
                lat_ref[block],
                key_up_ref[:, n * span : (n + 1) * span],
                preferred_element_type=jnp.float32,
            ).astype(jnp.bfloat16)

        def expand_values(n):
            values = lax.dot_general(
                turned_ref[n * span : (n + 1) * span, :],
                lat_ref[block],
                (((1,), (1,)), ((), ())),
                preferred_element_type=jnp.float32,
            ).astype(jnp.bfloat16)
            for head in range(2 * per):
                values_refs[n][head * head_rows : head * head_rows + VALUE_DIM, :] = values[
                    head * VALUE_DIM : (head + 1) * VALUE_DIM, :
                ]

        def product(at):
            pair, i = work[at]
            begin = tiles[i][0]
            within = (pair % per) * 2 * NOPE_DIM
            key_pair = jnp.concatenate(
                [key_refs[pair // per][:, within : within + 2 * NOPE_DIM], rot_ref[block]], axis=1
            )
            score = jnp.dot(
                key_pair, qbd_ref[pair, :, begin : begin + width], preferred_element_type=jnp.float32
            )
            if masked:
                column = lax.broadcasted_iota(jnp.int32, (queries, width), 1) + begin
                column = jnp.where(column >= queries, column - queries, column)
                visible = lax.broadcasted_iota(jnp.int32, (queries, width), 0) <= column
                score_refs[at % 2][:queries, :] = jnp.where(visible, score[:queries], far_below)
                score_refs[at % 2][queries:, :] = score[queries:]
            else:
                score_refs[at % 2][...] = score

        def soften(at):
            old_max = max_ref[at : at + 1, :]
            score = score_refs[at % 2]
            new_max = jnp.maximum(old_max, jnp.max(score[...], axis=0, keepdims=True))
            weight_refs[at % 2][...] = jnp.exp2(score[...] - new_max).astype(jnp.bfloat16)
            shrinks[at] = jnp.exp2(old_max - new_max)
            max_ref[at : at + 1, :] = new_max

        def weigh(at):
            pair, i = work[at]
            parts = tiles[i][1]
            head = 2 * (pair % per) + parts[0][0]
            fresh = jnp.dot(
                values_refs[pair // per][head * head_rows : (head + len(parts)) * head_rows, :],
                weight_refs[at % 2][...],
                preferred_element_type=jnp.float32,
            )
            if len(parts) > 1:
                fresh = jnp.concatenate(
                    [
                        fresh[n * head_rows : (n + 1) * head_rows, low:high]
                        for n, (_, low, high) in enumerate(parts)
                    ],
                    axis=1,
                )
            acc_ref[at] = acc_ref[at] * shrinks[at] + fresh

        share = per * len(tiles)
        expand_keys(0)
        product(0)
        expand_values(0)
        for at in range(len(work) + 1):
            ahead = (at + 3) // share
            if (at + 3) % share == 0 and 0 < ahead < parcels:
                expand_keys(ahead)
            ahead = (at + 1) // share
            if (at + 1) % share == 0 and 0 < ahead < parcels:
                expand_values(ahead)
            if at + 1 < len(work):
                product(at + 1)
            if at < len(work):
                soften(at)
            if at > 0:
                weigh(at - 1)

    if first:
        visit(0, True)

    @pl.loop(1 if first else 0, blocks)
    def each_block(block):
        low = 2 * block - (1 if first else 0)
        high = jnp.minimum(low + 1, slot - 1)

        @pl.when((vis_ref[low] > 0) | (vis_ref[high] > 0))
        def seen():
            visit(block, False)

    if last:
        for pair in range(pairs):
            pieces_of = ([], [])
            for i, (_, parts) in enumerate(tiles):
                done = acc_ref[pair * len(tiles) + i]
                done = done[:VALUE_DIM] / done[VALUE_DIM : VALUE_DIM + 1]
                for side, low, high in parts:
                    pieces_of[side].append(done[:, low:high])
            both = jnp.concatenate([jnp.concatenate(p, axis=1) for p in pieces_of], axis=0)
            out_ref[:, pair * 2 * VALUE_DIM : (pair + 1) * 2 * VALUE_DIM] = both.T.astype(out_ref.dtype)


def attention_stage(visible, queries_t, query_rot_t, key_up, value_up, slots, rows, groups,
                    own=None, state=None, last=False):
    first = own is not None
    heads = key_up.shape[1] // NOPE_DIM
    tok_rows = queries_t.shape[1]
    counts = [[p.shape[0] if p.ndim == 3 else 0 for p in s] for s in slots]
    total_blocks = sum(c[0] or 1 for c in counts) + (1 if first else 0)
    blocks = (total_blocks + 1) // 2
    width, tiles = tiles_of(tok_rows)
    tile_count = heads // 2 * len(tiles)
    extra = own if first else state
    consts = [queries_t, query_rot_t, key_up, value_up]
    flat = [p for s in slots for p in s]
    acc_shape = (tile_count, VALUE_DIM + SUM_ROWS, width)
    max_shape = (tile_count, width)
    parcels = max(1, heads // 4)
    keys = 2 * tok_rows
    scratch = (
        [
            pltpu.VMEM((blocks, keys, key_up.shape[0]), jnp.bfloat16),
            pltpu.VMEM((blocks, keys, 128), jnp.bfloat16),
            pltpu.VMEM((heads // 2, 256, 2 * tok_rows), jnp.bfloat16),
            pltpu.VMEM(value_up.shape[::-1], jnp.bfloat16),
        ]
        + [pltpu.VMEM((keys, width), jnp.float32)] * 2
        + [pltpu.VMEM((keys, width), jnp.bfloat16)] * 2
        + [pltpu.VMEM((keys, heads // parcels * NOPE_DIM), jnp.bfloat16)] * parcels
        + [pltpu.VMEM((heads // parcels * (VALUE_DIM + SUM_ROWS), keys), jnp.bfloat16)] * parcels
    )
    if last:
        out_shape = jax.ShapeDtypeStruct((tok_rows, heads * VALUE_DIM), jnp.bfloat16)
        scratch = [pltpu.VMEM(max_shape, jnp.float32), pltpu.VMEM(acc_shape, jnp.float32)] + scratch
    else:
        out_shape = (
            jax.ShapeDtypeStruct(max_shape, jnp.float32),
            jax.ShapeDtypeStruct(acc_shape, jnp.float32),
        )
    flops = 2 * total_blocks * tok_rows * tok_rows * heads * (256 + VALUE_DIM)
    in_vmem = pl.BlockSpec()
    return pl.pallas_call(
        functools.partial(attention_kernel, first, last, counts, rows, groups, heads),
        in_specs=[pl.BlockSpec(memory_space=pltpu.SMEM)] + [in_vmem] * (len(consts) + len(flat) + len(extra)),
        out_specs=in_vmem if last else (in_vmem, in_vmem),
        scratch_shapes=scratch,
        out_shape=out_shape,
        compiler_params=pltpu.CompilerParams(vmem_limit_bytes=24 * 1024 * 1024),
        cost_estimate=pl.CostEstimate(
            flops=flops, bytes_accessed=4 << 20, transcendentals=total_blocks * tok_rows * tok_rows * heads
        ),
        name="attention_first" if first else "attention_rest",
    )(visible, *consts, *flat, *extra)


def conv_kernel(rim, gated_ref, rim_ref, taps_ref, out_ref, padded_ref):
    rows, chans = gated_ref.shape
    padded_ref[:rim, :] = rim_ref[...].astype(jnp.float32)
    padded_ref[rim : rim + rows, :] = gated_ref[...].astype(jnp.float32)
    offset = rim - (KERNEL - 1)
    step = math.gcd(rows, 64)
    for lane in range(0, chans, 128):
        lanes = slice(lane, lane + 128)
        for row in range(0, rows, step):
            acc = jnp.zeros((step, 128), jnp.float32)
            for phase in range(8):
                taps = range(phase, KERNEL, 8)
                start = row + offset + phase
                part = padded_ref[start : start + step + 8 * (len(taps) - 1), lanes]
                for j, tap in enumerate(taps):
                    acc = acc + taps_ref[tap : tap + 1, lanes] * part[8 * j : 8 * j + step]
            out_ref[row : row + step, lanes] = acc


def convolve(gated, rim, taps):
    rows, chans = gated.shape
    rim_rows = rim.shape[0]
    return pl.pallas_call(
        functools.partial(conv_kernel, rim_rows),
        out_shape=jax.ShapeDtypeStruct((rows, chans), jnp.float32),
        scratch_shapes=[pltpu.VMEM((rim_rows + rows, chans), jnp.float32)],
        compiler_params=pltpu.CompilerParams(vmem_limit_bytes=6 * 1024 * 1024),
        cost_estimate=pl.CostEstimate(
            flops=2 * KERNEL * rows * chans * 50, bytes_accessed=6 * rows * chans, transcendentals=0
        ),
        name="conv",
    )(gated, rim, taps)


def shards(
    tokens,
    input_gain,
    query_weight,
    query_rot_weight,
    kv_down,
    rot_down,
    kv_gain,
    key_up,
    value_up,
    conv_value_weight,
    conv_gate_weight,
    conv_taps,
    conv_ln_gain,
    conv_ln_bias,
    att_out_gain,
    conv_out_gain,
    att_out_weight,
    conv_out_weight,
):
    tok_rows = tokens.shape[0]
    heads_here = key_up.shape[1] // NOPE_DIM
    tp_size, sp_size = lax.axis_size("tp"), lax.axis_size("sp")
    tp_index, sp_index = lax.axis_index("tp"), lax.axis_index("sp")
    f32, bf16 = jnp.float32, jnp.bfloat16

    positions = sp_index * tok_rows + jnp.arange(tok_rows, dtype=jnp.int32)
    cos_table, sine_table = rotary_tables(positions, ROT_DIM // 2)

    rows = tok_rows // tp_size
    rank = kv_down.shape[1]
    groups = max(
        g for g in range(1, rank // ROT_DIM + 1) if rows % g == 0 and (rows // g) % 8 == 0
    )
    scaled, row_scale, latent, own_rot, mine = front(
        jnp.full((1,), tp_index, jnp.int32),
        [tokens] + others(tokens, "tp"),
        input_gain[None, :],
        kv_down,
        rot_down.T,
        kv_gain[None, :],
        jnp.concatenate([cos_table, cos_table], axis=1),
        jnp.concatenate([-sine_table, sine_table], axis=1),
        groups,
    )

    plane = 4 if sp_size % 4 == 0 else 1
    high, low = sp_index // plane, sp_index % plane
    far = range(1, sp_size // plane)
    near, column = [], []
    for b in range(1, plane):
        near.append(swap_bits(mine, "sp", b))
    for s in far:
        column.append(shift_by(mine, "sp", plane * s))
    near_vis = [((low ^ b) < low).astype(jnp.int32) for b in range(1, plane)]
    column_vis = [(high >= s).astype(jnp.int32) for s in far]

    def with_pieces(arrays):
        return [[a] + others(a, "tp") for a in arrays]

    def project(weight):
        return jnp.dot(scaled, weight, preferred_element_type=f32)

    gated = (
        project(conv_value_weight) * row_scale * jax.nn.sigmoid(project(conv_gate_weight) * row_scale)
    ).astype(bf16)
    rim_rows = 32
    rim = shift_by(gated[tok_rows - rim_rows :], "sp", 1)
    scaled, gated = lax.optimization_barrier((scaled, gated))
    query_scale = row_scale * (math.log2(math.e) / math.sqrt(NOPE_DIM + ROT_DIM))
    queries_t = (project(query_weight) * query_scale).astype(bf16).T
    query_rot_t = (
        rotate_half(
            (project(query_rot_weight) * query_scale).reshape(tok_rows, heads_here, ROT_DIM),
            cos_table[:, None, :],
            sine_table[:, None, :],
        )
        .astype(bf16)
        .reshape(tok_rows, heads_here * ROT_DIM)
        .T
    )
    gated, rim, queries_t, query_rot_t = lax.optimization_barrier((gated, rim, queries_t, query_rot_t))
    conv_out = convolve(gated, rim, conv_taps)
    moments = total(jnp.stack([jnp.sum(conv_out, axis=1), jnp.sum(conv_out * conv_out, axis=1)]), "tp")
    mean_val = moments[0] / CONV_CH
    spread = moments[1] / CONV_CH - mean_val * mean_val
    normed = (conv_out - mean_val[:, None]) * lax.rsqrt(spread + norm_eps)[:, None]
    swished = jax.nn.silu(normed * conv_ln_gain[None, :] + conv_ln_bias[None, :])
    conv_sq = total(jnp.sum(swished * swished, axis=1)[None, :], "tp")[0]
    conv_mixed = (
        swished * lax.rsqrt(conv_sq / CONV_CH + norm_eps)[:, None] * conv_out_gain[None, :]
    ).astype(bf16)
    width = D_MODEL // tp_size

    def columns_of(device, weight):
        return lax.dynamic_slice_in_dim(weight, device * width, width, 1)

    def scatter(product):
        parts = []
        for d in range(1, tp_size):
            send = product((tp_index + tp_size - d) % tp_size).astype(bf16)
            parts.append(
                lax.ppermute(send, "tp", [((i + d) % tp_size, i) for i in range(tp_size)])
            )
        own = lax.optimization_barrier(product(tp_index))
        return own, parts

    own = (latent, own_rot)
    stage = functools.partial(
        attention_stage,
        queries_t=queries_t,
        query_rot_t=query_rot_t,
        key_up=key_up,
        value_up=value_up,
        rows=rows,
        groups=groups,
    )
    slots_one, vis_one = with_pieces(near + column), near_vis + column_vis
    slots_two, vis_two = [], []
    if plane == 4:
        if len(slots_one) % 2 == 0:
            slots_two, vis_two = slots_one[-1:], vis_one[-1:]
            slots_one, vis_one = slots_one[:-1], vis_one[:-1]
        column_all = jnp.stack(column)
        arrived = []
        for b in (1, 2):
            arrived.append(swap_bits(column_all, "sp", b))
        for s in far:
            arrived.append(shift_by(near[2], "sp", plane * s))
        state = stage(jnp.stack(vis_one), slots=slots_one, own=own)
        state, arrived, conv_mixed = lax.optimization_barrier((state, arrived, conv_mixed))
        slots_two = slots_two + with_pieces(arrived)
        vis_two = vis_two + column_vis * 3
    conv_own, conv_rest = scatter(
        lambda device: jnp.dot(
            conv_mixed, columns_of(device, conv_out_weight), preferred_element_type=f32
        )
    )
    conv_part = conv_own
    for part in conv_rest:
        conv_part = conv_part + part.astype(f32)
    if slots_two:
        state, conv_part = lax.optimization_barrier((state, conv_part))
        attended = stage(jnp.stack(vis_two), slots=slots_two, state=state, last=True)
    else:
        attended = stage(jnp.stack(vis_one), slots=slots_one, own=own, last=True)

    wide_att = attended.astype(f32)
    att_sq = total(jnp.sum(wide_att * wide_att, axis=1)[None, :], "tp")[0]
    gained = (wide_att * att_out_gain[None, :]).astype(bf16)
    att_part, att_rest = scatter(
        lambda device: jnp.dot(gained, columns_of(device, att_out_weight), preferred_element_type=f32)
    )
    for part in att_rest:
        att_part = att_part + part.astype(f32)
    return (att_part * lax.rsqrt(att_sq / ATT_WIDTH + norm_eps)[:, None] + conv_part).astype(bf16)


def solution(mesh):
    return jax.shard_map(
        shards,
        mesh=mesh,
        in_specs=(
            P("sp", "tp"),
            P(),
            P(None, "tp"),
            P(None, "tp"),
            P(),
            P(),
            P(),
            P(None, "tp"),
            P(None, "tp"),
            P(None, "tp"),
            P(None, "tp"),
            P(None, "tp"),
            P("tp"),
            P("tp"),
            P("tp"),
            P("tp"),
            P("tp", None),
            P("tp", None),
        ),
        out_specs=P("sp", "tp"),
        check_vma=False,
    )
```

```python
import functools
import math

import jax
import jax.numpy as jnp
from jax import lax
from jax.experimental import pallas as pl
from jax.experimental.pallas import tpu as pltpu
from jax.sharding import PartitionSpec as P


D_MODEL = 2048
NOPE_DIM = 64
ROT_DIM = 32
VALUE_DIM = 64
CONV_CH = 1024
KERNEL = 31
ATT_WIDTH = 1024


norm_eps = 1e-06
far_below = -1e30
rope_base = 10000.0
SUM_ROWS = 16


def rotary_tables(positions, half_dim):
    frequency = rope_base ** (-jnp.arange(half_dim, dtype=jnp.float32) / half_dim)
    angles = positions.astype(jnp.float32)[:, None] * frequency[None, :]
    return (jnp.cos(angles), jnp.sin(angles))


def rotate_half(values, cos_table, sine_table):
    half_dim = cos_table.shape[-1]
    front_half = values[..., :half_dim]
    back_half = values[..., half_dim:]
    return jnp.concatenate(
        [
            front_half * cos_table - back_half * sine_table,
            back_half * cos_table + front_half * sine_table,
        ],
        axis=-1,
    )


def shift_by(block, axis, distance):
    devices = range(lax.axis_size(axis))
    return lax.ppermute(block, axis, [(i, i + distance) for i in devices if i + distance in devices])


def swap_bits(block, axis, bits):
    return lax.ppermute(block, axis, [(i, i ^ bits) for i in range(lax.axis_size(axis))])


def others(block, axis):
    size = lax.axis_size(axis)
    return [
        lax.ppermute(block, axis, [((i + d) % size, i) for i in range(size)])
        for d in range(1, size)
    ]


def total(block, axis):
    for part in others(block, axis):
        block = block + part
    return block


def front_kernel(pieces, rows, groups, index_ref, *refs):
    token_refs, refs = refs[:pieces], refs[pieces:]
    gain_ref, down_ref, rot_down_ref, kv_gain_ref, cos_ref, sin_ref = refs[:6]
    scaled_ref, scale_ref, lat_ref, rot_ref, send_ref, wide_rot_ref = refs[6:]
    me = index_ref[0]
    tok_rows, width = token_refs[0].shape
    squares = jnp.zeros((tok_rows, 128), jnp.float32)
    for d, ref in enumerate(token_refs):
        begin = lax.rem(me + d, pieces) * width
        for col in range(0, width, 128):
            at = pl.ds(pl.multiple_of(begin + col, 128), 128)
            values = ref[:, col : col + 128].astype(jnp.float32)
            scaled_ref[:, at] = (values * gain_ref[:, at]).astype(jnp.bfloat16)
            squares = squares + values * values
    row_scale = lax.rsqrt(jnp.sum(squares, axis=1, keepdims=True) / D_MODEL + norm_eps)
    scale_ref[...] = row_scale
    raw = jnp.dot(scaled_ref[...], down_ref[...], preferred_element_type=jnp.float32)
    half = ROT_DIM // 2
    turned = jnp.concatenate(
        [rot_down_ref[...], rot_down_ref[half:, :], rot_down_ref[:half, :]], axis=0
    )
    both = (
        lax.dot_general(
            scaled_ref[...], turned, (((1,), (1,)), ((), ())), preferred_element_type=jnp.float32
        )
        * row_scale
    )
    mean = jnp.mean(raw * raw, axis=1, keepdims=True)
    lat_ref[...] = (raw * lax.rsqrt(mean + norm_eps) * kv_gain_ref[...]).astype(jnp.bfloat16)
    rot = both[:, :ROT_DIM] * cos_ref[...] + both[:, ROT_DIM : 2 * ROT_DIM] * sin_ref[...]
    rot = jnp.concatenate([rot, jnp.zeros((tok_rows, 128 - ROT_DIM), jnp.float32)], axis=1)
    wide_rot_ref[...] = rot
    rot_ref[...] = rot.astype(jnp.bfloat16)
    start = me * rows
    send_ref[:rows, :] = lat_ref[pl.ds(pl.multiple_of(start, 16), rows), :]
    height = rows // groups
    packed = [
        wide_rot_ref[pl.ds(pl.multiple_of(start + g * height, 8), height), :][:, :ROT_DIM]
        for g in range(groups)
    ]
    rank = lat_ref.shape[1]
    if groups * ROT_DIM < rank:
        packed.append(jnp.zeros((height, rank - groups * ROT_DIM), jnp.float32))
    packed = jnp.concatenate(packed, axis=1)
    spare = send_ref.shape[0] - rows - height
    if spare:
        packed = jnp.concatenate([packed, jnp.zeros((spare, rank), jnp.float32)], axis=0)
    send_ref[rows:, :] = packed.astype(jnp.bfloat16)


def front(index, pieces, gain, down, rot_down, kv_gain, cos, sin, groups):
    tok_rows, width = pieces[0].shape
    rank = down.shape[1]
    rows = tok_rows // len(pieces)
    height = rows // groups
    model = width * len(pieces)
    in_vmem = pl.BlockSpec()
    args = list(pieces) + [gain, down, rot_down, kv_gain, cos, sin]
    return pl.pallas_call(
        functools.partial(front_kernel, len(pieces), rows, groups),
        in_specs=[pl.BlockSpec(memory_space=pltpu.SMEM)] + [in_vmem] * len(args),
        out_specs=(in_vmem,) * 5,
        out_shape=(
            jax.ShapeDtypeStruct((tok_rows, model), jnp.bfloat16),
            jax.ShapeDtypeStruct((tok_rows, 1), jnp.float32),
            jax.ShapeDtypeStruct((tok_rows, rank), jnp.bfloat16),
            jax.ShapeDtypeStruct((tok_rows, 128), jnp.bfloat16),
            jax.ShapeDtypeStruct((rows + height + -height % 16, rank), jnp.bfloat16),
        ),
        scratch_shapes=[pltpu.VMEM((tok_rows, 128), jnp.float32)],
        compiler_params=pltpu.CompilerParams(vmem_limit_bytes=16 * 1024 * 1024),
        cost_estimate=pl.CostEstimate(
            flops=2 * tok_rows * model * 512, bytes_accessed=8 << 20, transcendentals=tok_rows
        ),
        name="front",
    )(index, *args)


def tiles_of(queries):
    width = 256 if (2 * queries) % 256 == 0 else queries
    out = []
    for start in range(0, 2 * queries, width):
        parts = []
        for side in range(2):
            low = max(start, side * queries)
            high = min(start + width, (side + 1) * queries)
            if low < high:
                parts.append((side, low - start, high - start))
        out.append((start, parts))
    return width, out


def attention_kernel(first, last, counts, rows, groups, heads, vis_ref, *refs):
    refs = list(refs)
    qt_ref, qrt_ref, key_up_ref, value_up_ref = refs[:4]
    refs = refs[4:]
    pieces = len(counts[0])
    sources = []
    for _ in counts:
        sources.append(refs[:pieces])
        refs = refs[pieces:]
    if first:
        (own_lat_ref, own_rot_ref), refs = refs[:2], refs[2:]
    else:
        (max_in, acc_in), refs = refs[:2], refs[2:]
    if last:
        (out_ref, max_ref, acc_ref), refs = refs[:3], refs[3:]
    else:
        (max_ref, acc_ref), refs = refs[:2], refs[2:]
    lat_ref, rot_ref, qbd_ref, score_refs, weight_refs, refs = (
        refs[0], refs[1], refs[2], refs[3:5], refs[5:7], refs[7:]
    )
    pairs = heads // 2
    parcels = max(1, pairs // 2)
    key_refs, values_refs = refs[:parcels], refs[parcels:]
    per = pairs // parcels
    queries = qt_ref.shape[1]
    width, tiles = tiles_of(queries)
    head_rows = VALUE_DIM + SUM_ROWS
    blocks = lat_ref.shape[0]
    bias_row = 2 * NOPE_DIM + ROT_DIM

    qbd_ref[...] = jnp.zeros_like(qbd_ref)
    for pair in range(pairs):
        qbd_ref[pair, bias_row : bias_row + 16, :] = (
            lax.broadcasted_iota(jnp.int32, (16, 2 * queries), 0) == 0
        ).astype(jnp.bfloat16)
        for side in range(2):
            head = 2 * pair + side
            columns = slice(side * queries, (side + 1) * queries)
            qbd_ref[pair, side * NOPE_DIM : (side + 1) * NOPE_DIM, columns] = qt_ref[
                head * NOPE_DIM : (head + 1) * NOPE_DIM, :
            ]
            qbd_ref[pair, 2 * NOPE_DIM : 2 * NOPE_DIM + ROT_DIM, columns] = qrt_ref[
                head * ROT_DIM : (head + 1) * ROT_DIM, :
            ]
    for ref in values_refs:
        ref[...] = jnp.ones_like(ref)
    if first:
        max_ref[...] = jnp.full_like(max_ref, far_below)
        acc_ref[...] = jnp.zeros_like(acc_ref)
        lat_ref[0, :queries, :] = own_lat_ref[...]
        rot_ref[0, :queries, :] = own_rot_ref[...]
    else:
        max_ref[...] = max_in[...]
        acc_ref[...] = acc_in[...]

    at = 1 if first else 0
    slot = 0
    is_bias = lax.broadcasted_iota(jnp.int32, (queries, 128), 1) == ROT_DIM
    for source, several in zip(sources, counts):
        for index in range(several[0] or 1):
            rots = []
            base = (at % 2) * queries
            for n, ref in enumerate(source):
                view = ref.at[index] if several[0] else ref
                lat_ref[at // 2, base + n * rows : base + (n + 1) * rows, :] = view[:rows, :]
                packed = view[rows:, :].astype(jnp.float32)[: rows // groups]
                rots += [packed[:, g * ROT_DIM : (g + 1) * ROT_DIM] for g in range(groups)]
            rot = jnp.concatenate(rots, axis=0)
            rot = jnp.concatenate([rot, jnp.zeros((queries, 128 - ROT_DIM), jnp.float32)], axis=1)
            bias = jnp.where(vis_ref[slot] > 0, 0.0, far_below)
            rot_ref[at // 2, base : base + queries, :] = jnp.where(is_bias, bias, rot).astype(jnp.bfloat16)
            at += 1
            slot += 1
    if at % 2:
        lat_ref[at // 2, queries:, :] = jnp.zeros((queries, lat_ref.shape[2]), jnp.bfloat16)
        rot_ref[at // 2, queries:, :] = jnp.where(is_bias, far_below, 0.0).astype(jnp.bfloat16)

    def visit(block, masked):
        span = per * 2 * NOPE_DIM
        work = [(pair, i) for pair in range(pairs) for i in range(len(tiles))]
        shrinks = {}

        def expand_keys(n):
            key_refs[n][...] = jnp.dot(
                lat_ref[block],
                key_up_ref[:, n * span : (n + 1) * span],
                preferred_element_type=jnp.float32,
            ).astype(jnp.bfloat16)

        def expand_values(n):
            values = lax.dot_general(
                value_up_ref[n * span : (n + 1) * span, :],
                lat_ref[block],
                (((1,), (1,)), ((), ())),
                preferred_element_type=jnp.float32,
            ).astype(jnp.bfloat16)
            for head in range(2 * per):
                values_refs[n][head * head_rows : head * head_rows + VALUE_DIM, :] = values[
                    head * VALUE_DIM : (head + 1) * VALUE_DIM, :
                ]

        def product(at):
            pair, i = work[at]
            begin = tiles[i][0]
            within = (pair % per) * 2 * NOPE_DIM
            key_pair = jnp.concatenate(
                [key_refs[pair // per][:, within : within + 2 * NOPE_DIM], rot_ref[block]], axis=1
            )
            score = jnp.dot(
                key_pair, qbd_ref[pair, :, begin : begin + width], preferred_element_type=jnp.float32
            )
            if masked:
                column = lax.broadcasted_iota(jnp.int32, (queries, width), 1) + begin
                column = jnp.where(column >= queries, column - queries, column)
                visible = lax.broadcasted_iota(jnp.int32, (queries, width), 0) <= column
                score_refs[at % 2][:queries, :] = jnp.where(visible, score[:queries], far_below)
                score_refs[at % 2][queries:, :] = score[queries:]
            else:
                score_refs[at % 2][...] = score

        def soften(at):
            old_max = max_ref[at : at + 1, :]
            score = score_refs[at % 2]
            new_max = jnp.maximum(old_max, jnp.max(score[...], axis=0, keepdims=True))
            weight_refs[at % 2][...] = jnp.exp2(score[...] - new_max).astype(jnp.bfloat16)
            shrinks[at] = jnp.exp2(old_max - new_max)
            max_ref[at : at + 1, :] = new_max

        def weigh(at):
            pair, i = work[at]
            parts = tiles[i][1]
            head = 2 * (pair % per) + parts[0][0]
            fresh = jnp.dot(
                values_refs[pair // per][head * head_rows : (head + len(parts)) * head_rows, :],
                weight_refs[at % 2][...],
                preferred_element_type=jnp.float32,
            )
            if len(parts) > 1:
                fresh = jnp.concatenate(
                    [
                        fresh[n * head_rows : (n + 1) * head_rows, low:high]
                        for n, (_, low, high) in enumerate(parts)
                    ],
                    axis=1,
                )
            acc_ref[at] = acc_ref[at] * shrinks[at] + fresh

        share = per * len(tiles)
        expand_keys(0)
        product(0)
        expand_values(0)
        for at in range(len(work) + 1):
            ahead = (at + 3) // share
            if (at + 3) % share == 0 and 0 < ahead < parcels:
                expand_keys(ahead)
            ahead = (at + 1) // share
            if (at + 1) % share == 0 and 0 < ahead < parcels:
                expand_values(ahead)
            if at + 1 < len(work):
                product(at + 1)
            if at < len(work):
                soften(at)
            if at > 0:
                weigh(at - 1)

    if first:
        visit(0, True)

    @pl.loop(1 if first else 0, blocks)
    def each_block(block):
        low = 2 * block - (1 if first else 0)
        high = jnp.minimum(low + 1, slot - 1)

        @pl.when((vis_ref[low] > 0) | (vis_ref[high] > 0))
        def seen():
            visit(block, False)

    if last:
        for pair in range(pairs):
            pieces_of = ([], [])
            for i, (_, parts) in enumerate(tiles):
                done = acc_ref[pair * len(tiles) + i]
                done = done[:VALUE_DIM] / done[VALUE_DIM : VALUE_DIM + 1]
                for side, low, high in parts:
                    pieces_of[side].append(done[:, low:high])
            both = jnp.concatenate([jnp.concatenate(p, axis=1) for p in pieces_of], axis=0)
            out_ref[:, pair * 2 * VALUE_DIM : (pair + 1) * 2 * VALUE_DIM] = both.T.astype(out_ref.dtype)


def attention_stage(visible, queries_t, query_rot_t, key_up, value_up, slots, rows, groups,
                    own=None, state=None, last=False):
    first = own is not None
    heads = key_up.shape[1] // NOPE_DIM
    tok_rows = queries_t.shape[1]
    counts = [[p.shape[0] if p.ndim == 3 else 0 for p in s] for s in slots]
    total_blocks = sum(c[0] or 1 for c in counts) + (1 if first else 0)
    blocks = (total_blocks + 1) // 2
    width, tiles = tiles_of(tok_rows)
    tile_count = heads // 2 * len(tiles)
    extra = own if first else state
    consts = [queries_t, query_rot_t, key_up, value_up]
    flat = [p for s in slots for p in s]
    acc_shape = (tile_count, VALUE_DIM + SUM_ROWS, width)
    max_shape = (tile_count, width)
    parcels = max(1, heads // 4)
    keys = 2 * tok_rows
    scratch = (
        [
            pltpu.VMEM((blocks, keys, key_up.shape[0]), jnp.bfloat16),
            pltpu.VMEM((blocks, keys, 128), jnp.bfloat16),
            pltpu.VMEM((heads // 2, 256, 2 * tok_rows), jnp.bfloat16),
        ]
        + [pltpu.VMEM((keys, width), jnp.float32)] * 2
        + [pltpu.VMEM((keys, width), jnp.bfloat16)] * 2
        + [pltpu.VMEM((keys, heads // parcels * NOPE_DIM), jnp.bfloat16)] * parcels
        + [pltpu.VMEM((heads // parcels * (VALUE_DIM + SUM_ROWS), keys), jnp.bfloat16)] * parcels
    )
    if last:
        out_shape = jax.ShapeDtypeStruct((tok_rows, heads * VALUE_DIM), jnp.bfloat16)
        scratch = [pltpu.VMEM(max_shape, jnp.float32), pltpu.VMEM(acc_shape, jnp.float32)] + scratch
    else:
        out_shape = (
            jax.ShapeDtypeStruct(max_shape, jnp.float32),
            jax.ShapeDtypeStruct(acc_shape, jnp.float32),
        )
    flops = 2 * total_blocks * tok_rows * tok_rows * heads * (256 + VALUE_DIM)
    in_vmem = pl.BlockSpec()
    return pl.pallas_call(
        functools.partial(attention_kernel, first, last, counts, rows, groups, heads),
        in_specs=[pl.BlockSpec(memory_space=pltpu.SMEM)] + [in_vmem] * (len(consts) + len(flat) + len(extra)),
        out_specs=in_vmem if last else (in_vmem, in_vmem),
        scratch_shapes=scratch,
        out_shape=out_shape,
        compiler_params=pltpu.CompilerParams(vmem_limit_bytes=24 * 1024 * 1024),
        cost_estimate=pl.CostEstimate(
            flops=flops, bytes_accessed=4 << 20, transcendentals=total_blocks * tok_rows * tok_rows * heads
        ),
        name="attention_first" if first else "attention_rest",
    )(visible, *consts, *flat, *extra)


def conv_kernel(rim, gated_ref, rim_ref, taps_ref, out_ref, padded_ref):
    rows, chans = gated_ref.shape
    padded_ref[:rim, :] = rim_ref[...].astype(jnp.float32)
    padded_ref[rim : rim + rows, :] = gated_ref[...].astype(jnp.float32)
    offset = rim - (KERNEL - 1)
    step = math.gcd(rows, 64)
    for lane in range(0, chans, 128):
        lanes = slice(lane, lane + 128)
        for row in range(0, rows, step):
            acc = jnp.zeros((step, 128), jnp.float32)
            for phase in range(8):
                taps = range(phase, KERNEL, 8)
                start = row + offset + phase
                part = padded_ref[start : start + step + 8 * (len(taps) - 1), lanes]
                for j, tap in enumerate(taps):
                    acc = acc + taps_ref[tap : tap + 1, lanes] * part[8 * j : 8 * j + step]
            out_ref[row : row + step, lanes] = acc


def convolve(gated, rim, taps):
    rows, chans = gated.shape
    rim_rows = rim.shape[0]
    return pl.pallas_call(
        functools.partial(conv_kernel, rim_rows),
        out_shape=jax.ShapeDtypeStruct((rows, chans), jnp.float32),
        scratch_shapes=[pltpu.VMEM((rim_rows + rows, chans), jnp.float32)],
        compiler_params=pltpu.CompilerParams(vmem_limit_bytes=6 * 1024 * 1024),
        cost_estimate=pl.CostEstimate(
            flops=2 * KERNEL * rows * chans * 50, bytes_accessed=6 * rows * chans, transcendentals=0
        ),
        name="conv",
    )(gated, rim, taps)


def shards(
    tokens,
    input_gain,
    query_weight,
    query_rot_weight,
    kv_down,
    rot_down,
    kv_gain,
    key_up,
    value_up,
    conv_value_weight,
    conv_gate_weight,
    conv_taps,
    conv_ln_gain,
    conv_ln_bias,
    att_out_gain,
    conv_out_gain,
    att_out_weight,
    conv_out_weight,
):
    tok_rows = tokens.shape[0]
    heads_here = key_up.shape[1] // NOPE_DIM
    tp_size, sp_size = lax.axis_size("tp"), lax.axis_size("sp")
    tp_index, sp_index = lax.axis_index("tp"), lax.axis_index("sp")
    f32, bf16 = jnp.float32, jnp.bfloat16

    positions = sp_index * tok_rows + jnp.arange(tok_rows, dtype=jnp.int32)
    cos_table, sine_table = rotary_tables(positions, ROT_DIM // 2)

    rows = tok_rows // tp_size
    rank = kv_down.shape[1]
    groups = max(
        g for g in range(1, rank // ROT_DIM + 1) if rows % g == 0 and (rows // g) % 8 == 0
    )

    def near_by(array):
        return jnp.maximum(array, jnp.finfo(array.dtype).min)

    token_pieces = others(tokens, "tp")
    key_up = near_by(key_up)
    value_up = value_up.T
    scaled, row_scale, latent, own_rot, mine = front(
        jnp.full((1,), tp_index, jnp.int32),
        [near_by(tokens)] + token_pieces,
        near_by(input_gain)[None, :],
        near_by(kv_down),
        near_by(rot_down.T),
        near_by(kv_gain)[None, :],
        jnp.concatenate([cos_table, cos_table], axis=1),
        jnp.concatenate([-sine_table, sine_table], axis=1),
        groups,
    )

    plane = 4 if sp_size % 4 == 0 else 1
    high, low = sp_index // plane, sp_index % plane
    far = range(1, sp_size // plane)
    near, column = [], []
    for b in range(1, plane):
        near.append(swap_bits(mine, "sp", b))
    for s in far:
        column.append(shift_by(mine, "sp", plane * s))
    near_vis = [((low ^ b) < low).astype(jnp.int32) for b in range(1, plane)]
    column_vis = [(high >= s).astype(jnp.int32) for s in far]

    def with_pieces(arrays):
        return [[a] + others(a, "tp") for a in arrays]

    def project(weight):
        return jnp.dot(scaled, weight, preferred_element_type=f32)

    gated = (
        project(conv_value_weight) * row_scale * jax.nn.sigmoid(project(conv_gate_weight) * row_scale)
    ).astype(bf16)
    rim_rows = 32
    rim = shift_by(gated[tok_rows - rim_rows :], "sp", 1)
    scaled, gated = lax.optimization_barrier((scaled, gated))
    query_scale = row_scale * (math.log2(math.e) / math.sqrt(NOPE_DIM + ROT_DIM))
    queries_t = (project(query_weight) * query_scale).astype(bf16).T
    query_rot_t = (
        rotate_half(
            (project(query_rot_weight) * query_scale).reshape(tok_rows, heads_here, ROT_DIM),
            cos_table[:, None, :],
            sine_table[:, None, :],
        )
        .astype(bf16)
        .reshape(tok_rows, heads_here * ROT_DIM)
        .T
    )
    gated, rim, queries_t, query_rot_t = lax.optimization_barrier((gated, rim, queries_t, query_rot_t))
    conv_out = convolve(gated, rim, conv_taps)
    moments = total(jnp.stack([jnp.sum(conv_out, axis=1), jnp.sum(conv_out * conv_out, axis=1)]), "tp")
    mean_val = moments[0] / CONV_CH
    spread = moments[1] / CONV_CH - mean_val * mean_val
    normed = (conv_out - mean_val[:, None]) * lax.rsqrt(spread + norm_eps)[:, None]
    swished = jax.nn.silu(normed * conv_ln_gain[None, :] + conv_ln_bias[None, :])
    conv_sq = total(jnp.sum(swished * swished, axis=1)[None, :], "tp")[0]
    conv_mixed = (
        swished * lax.rsqrt(conv_sq / CONV_CH + norm_eps)[:, None] * conv_out_gain[None, :]
    ).astype(bf16)
    width = D_MODEL // tp_size

    def columns_of(device, weight):
        return lax.dynamic_slice_in_dim(weight, device * width, width, 1)

    def scatter(product):
        parts = []
        for d in range(1, tp_size):
            send = product((tp_index + tp_size - d) % tp_size).astype(bf16)
            parts.append(
                lax.ppermute(send, "tp", [((i + d) % tp_size, i) for i in range(tp_size)])
            )
        own = lax.optimization_barrier(product(tp_index))
        return own, parts

    own = (latent, own_rot)
    stage = functools.partial(
        attention_stage,
        queries_t=queries_t,
        query_rot_t=query_rot_t,
        key_up=key_up,
        value_up=value_up,
        rows=rows,
        groups=groups,
    )
    slots_one, vis_one = with_pieces(near + column), near_vis + column_vis
    slots_two, vis_two = [], []
    if plane == 4:
        if len(slots_one) % 2 == 0:
            slots_two, vis_two = slots_one[-1:], vis_one[-1:]
            slots_one, vis_one = slots_one[:-1], vis_one[:-1]
        column_all = jnp.stack(column)
        arrived = []
        for b in (1, 2):
            arrived.append(swap_bits(column_all, "sp", b))
        for s in far:
            arrived.append(shift_by(near[2], "sp", plane * s))
        state = stage(jnp.stack(vis_one), slots=slots_one, own=own)
        state, arrived, conv_mixed = lax.optimization_barrier((state, arrived, conv_mixed))
        slots_two = slots_two + with_pieces(arrived)
        vis_two = vis_two + column_vis * 3
    conv_own, conv_rest = scatter(
        lambda device: jnp.dot(
            conv_mixed, columns_of(device, conv_out_weight), preferred_element_type=f32
        )
    )
    conv_part = conv_own
    for part in conv_rest:
        conv_part = conv_part + part.astype(f32)
    if slots_two:
        state, conv_part = lax.optimization_barrier((state, conv_part))
        attended = stage(jnp.stack(vis_two), slots=slots_two, state=state, last=True)
    else:
        attended = stage(jnp.stack(vis_one), slots=slots_one, own=own, last=True)

    wide_att = attended.astype(f32)
    att_sq = total(jnp.sum(wide_att * wide_att, axis=1)[None, :], "tp")[0]
    gained = (wide_att * att_out_gain[None, :]).astype(bf16)
    att_part, att_rest = scatter(
        lambda device: jnp.dot(gained, columns_of(device, att_out_weight), preferred_element_type=f32)
    )
    for part in att_rest:
        att_part = att_part + part.astype(f32)
    return (att_part * lax.rsqrt(att_sq / ATT_WIDTH + norm_eps)[:, None] + conv_part).astype(bf16)


def solution(mesh):
    return jax.shard_map(
        shards,
        mesh=mesh,
        in_specs=(
            P("sp", "tp"),
            P(),
            P(None, "tp"),
            P(None, "tp"),
            P(),
            P(),
            P(),
            P(None, "tp"),
            P(None, "tp"),
            P(None, "tp"),
            P(None, "tp"),
            P(None, "tp"),
            P("tp"),
            P("tp"),
            P("tp"),
            P("tp"),
            P("tp", None),
            P("tp", None),
        ),
        out_specs=P("sp", "tp"),
        check_vma=False,
    )
```

```python
import functools
import math

import jax
import jax.numpy as jnp
from jax import lax
from jax.experimental import pallas as pl
from jax.experimental.pallas import tpu as pltpu
from jax.sharding import PartitionSpec as P


D_MODEL = 2048
NOPE_DIM = 64
ROT_DIM = 32
VALUE_DIM = 64
CONV_CH = 1024
KERNEL = 31
ATT_WIDTH = 1024


norm_eps = 1e-06
far_below = -1e30
rope_base = 10000.0
SUM_ROWS = 16


def rotary_tables(positions, half_dim):
    frequency = rope_base ** (-jnp.arange(half_dim, dtype=jnp.float32) / half_dim)
    angles = positions.astype(jnp.float32)[:, None] * frequency[None, :]
    return (jnp.cos(angles), jnp.sin(angles))


def rotate_half(values, cos_table, sine_table):
    half_dim = cos_table.shape[-1]
    front_half = values[..., :half_dim]
    back_half = values[..., half_dim:]
    return jnp.concatenate(
        [
            front_half * cos_table - back_half * sine_table,
            back_half * cos_table + front_half * sine_table,
        ],
        axis=-1,
    )


def shift_by(block, axis, distance):
    devices = range(lax.axis_size(axis))
    return lax.ppermute(block, axis, [(i, i + distance) for i in devices if i + distance in devices])


def swap_bits(block, axis, bits):
    return lax.ppermute(block, axis, [(i, i ^ bits) for i in range(lax.axis_size(axis))])


def others(block, axis):
    size = lax.axis_size(axis)
    return [
        lax.ppermute(block, axis, [((i + d) % size, i) for i in range(size)])
        for d in range(1, size)
    ]


def total(block, axis):
    for part in others(block, axis):
        block = block + part
    return block


def front_kernel(pieces, rows, groups, index_ref, *refs):
    token_refs, refs = refs[:pieces], refs[pieces:]
    gain_ref, down_ref, rot_down_ref, kv_gain_ref, cos_ref, sin_ref = refs[:6]
    scaled_ref, scale_ref, lat_ref, rot_ref, send_ref, wide_rot_ref = refs[6:]
    me = index_ref[0]
    tok_rows, width = token_refs[0].shape
    squares = jnp.zeros((tok_rows, 128), jnp.float32)
    for d, ref in enumerate(token_refs):
        begin = lax.rem(me + d, pieces) * width
        for col in range(0, width, 128):
            at = pl.ds(pl.multiple_of(begin + col, 128), 128)
            values = ref[:, col : col + 128].astype(jnp.float32)
            scaled_ref[:, at] = (values * gain_ref[:, at]).astype(jnp.bfloat16)
            squares = squares + values * values
    row_scale = lax.rsqrt(jnp.sum(squares, axis=1, keepdims=True) / D_MODEL + norm_eps)
    scale_ref[...] = row_scale
    raw = jnp.dot(scaled_ref[...], down_ref[...], preferred_element_type=jnp.float32)
    half = ROT_DIM // 2
    turned = jnp.concatenate(
        [rot_down_ref[...], rot_down_ref[half:, :], rot_down_ref[:half, :]], axis=0
    )
    both = (
        lax.dot_general(
            scaled_ref[...], turned, (((1,), (1,)), ((), ())), preferred_element_type=jnp.float32
        )
        * row_scale
    )
    mean = jnp.mean(raw * raw, axis=1, keepdims=True)
    lat_ref[...] = (raw * lax.rsqrt(mean + norm_eps) * kv_gain_ref[...]).astype(jnp.bfloat16)
    rot = both[:, :ROT_DIM] * cos_ref[...] + both[:, ROT_DIM : 2 * ROT_DIM] * sin_ref[...]
    rot = jnp.concatenate([rot, jnp.zeros((tok_rows, 128 - ROT_DIM), jnp.float32)], axis=1)
    wide_rot_ref[...] = rot
    rot_ref[...] = rot.astype(jnp.bfloat16)
    start = me * rows
    send_ref[:rows, :] = lat_ref[pl.ds(pl.multiple_of(start, 16), rows), :]
    height = rows // groups
    packed = [
        wide_rot_ref[pl.ds(pl.multiple_of(start + g * height, 8), height), :][:, :ROT_DIM]
        for g in range(groups)
    ]
    rank = lat_ref.shape[1]
    if groups * ROT_DIM < rank:
        packed.append(jnp.zeros((height, rank - groups * ROT_DIM), jnp.float32))
    packed = jnp.concatenate(packed, axis=1)
    spare = send_ref.shape[0] - rows - height
    if spare:
        packed = jnp.concatenate([packed, jnp.zeros((spare, rank), jnp.float32)], axis=0)
    send_ref[rows:, :] = packed.astype(jnp.bfloat16)


def front(index, pieces, gain, down, rot_down, kv_gain, cos, sin, groups):
    tok_rows, width = pieces[0].shape
    rank = down.shape[1]
    rows = tok_rows // len(pieces)
    height = rows // groups
    model = width * len(pieces)
    in_vmem = pl.BlockSpec()
    args = list(pieces) + [gain, down, rot_down, kv_gain, cos, sin]
    return pl.pallas_call(
        functools.partial(front_kernel, len(pieces), rows, groups),
        in_specs=[pl.BlockSpec(memory_space=pltpu.SMEM)] + [in_vmem] * len(args),
        out_specs=(in_vmem,) * 5,
        out_shape=(
            jax.ShapeDtypeStruct((tok_rows, model), jnp.bfloat16),
            jax.ShapeDtypeStruct((tok_rows, 1), jnp.float32),
            jax.ShapeDtypeStruct((tok_rows, rank), jnp.bfloat16),
            jax.ShapeDtypeStruct((tok_rows, 128), jnp.bfloat16),
            jax.ShapeDtypeStruct((rows + height + -height % 16, rank), jnp.bfloat16),
        ),
        scratch_shapes=[pltpu.VMEM((tok_rows, 128), jnp.float32)],
        compiler_params=pltpu.CompilerParams(vmem_limit_bytes=16 * 1024 * 1024),
        cost_estimate=pl.CostEstimate(
            flops=2 * tok_rows * model * 512, bytes_accessed=8 << 20, transcendentals=tok_rows
        ),
        name="front",
    )(index, *args)


def tiles_of(queries):
    width = 256 if (2 * queries) % 256 == 0 else queries
    out = []
    for start in range(0, 2 * queries, width):
        parts = []
        for side in range(2):
            low = max(start, side * queries)
            high = min(start + width, (side + 1) * queries)
            if low < high:
                parts.append((side, low - start, high - start))
        out.append((start, parts))
    return width, out


def attention_kernel(first, last, counts, order, rows, groups, heads, vis_ref, *refs):
    refs = list(refs)
    qt_ref, qrt_ref, key_up_ref, value_up_ref = refs[:4]
    refs = refs[4:]
    pieces = len(counts[0])
    sources = []
    for _ in counts:
        sources.append(refs[:pieces])
        refs = refs[pieces:]
    if first:
        (own_lat_ref, own_rot_ref), refs = refs[:2], refs[2:]
    else:
        (max_in, acc_in), refs = refs[:2], refs[2:]
    if last:
        (out_ref, max_ref, acc_ref), refs = refs[:3], refs[3:]
    else:
        (max_ref, acc_ref), refs = refs[:2], refs[2:]
    lat_ref, rot_ref, qbd_ref, score_refs, weight_refs, refs = (
        refs[0], refs[1], refs[2], refs[3:5], refs[5:7], refs[7:]
    )
    pairs = heads // 2
    parcels = max(1, pairs // 2)
    key_refs, values_refs = refs[:parcels], refs[parcels:]
    per = pairs // parcels
    queries = qt_ref.shape[1]
    width, tiles = tiles_of(queries)
    head_rows = VALUE_DIM + SUM_ROWS
    blocks = lat_ref.shape[0]
    bias_row = 2 * NOPE_DIM + ROT_DIM

    qbd_ref[...] = jnp.zeros_like(qbd_ref)
    for pair in range(pairs):
        qbd_ref[pair, bias_row : bias_row + 16, :] = (
            lax.broadcasted_iota(jnp.int32, (16, 2 * queries), 0) == 0
        ).astype(jnp.bfloat16)
        for side in range(2):
            head = 2 * pair + side
            columns = slice(side * queries, (side + 1) * queries)
            qbd_ref[pair, side * NOPE_DIM : (side + 1) * NOPE_DIM, columns] = qt_ref[
                head * NOPE_DIM : (head + 1) * NOPE_DIM, :
            ]
            qbd_ref[pair, 2 * NOPE_DIM : 2 * NOPE_DIM + ROT_DIM, columns] = qrt_ref[
                head * ROT_DIM : (head + 1) * ROT_DIM, :
            ]
    for ref in values_refs:
        ref[...] = jnp.ones_like(ref)
    if first:
        max_ref[...] = jnp.full_like(max_ref, far_below)
        acc_ref[...] = jnp.zeros_like(acc_ref)
        lat_ref[0, :queries, :] = own_lat_ref[...]
        rot_ref[0, :queries, :] = own_rot_ref[...]
    else:
        max_ref[...] = max_in[...]
        acc_ref[...] = acc_in[...]

    at = 1 if first else 0
    slot = 0
    is_bias = lax.broadcasted_iota(jnp.int32, (queries, 128), 1) == ROT_DIM
    for place, index in order:
        rots = []
        base = (at % 2) * queries
        for n, ref in enumerate(sources[place]):
            view = ref.at[index] if counts[place][0] else ref
            lat_ref[at // 2, base + n * rows : base + (n + 1) * rows, :] = view[:rows, :]
            packed = view[rows:, :].astype(jnp.float32)[: rows // groups]
            rots += [packed[:, g * ROT_DIM : (g + 1) * ROT_DIM] for g in range(groups)]
        rot = jnp.concatenate(rots, axis=0)
        rot = jnp.concatenate([rot, jnp.zeros((queries, 128 - ROT_DIM), jnp.float32)], axis=1)
        bias = jnp.where(vis_ref[slot] > 0, 0.0, far_below)
        rot_ref[at // 2, base : base + queries, :] = jnp.where(is_bias, bias, rot).astype(jnp.bfloat16)
        at += 1
        slot += 1
    if at % 2:
        lat_ref[at // 2, queries:, :] = jnp.zeros((queries, lat_ref.shape[2]), jnp.bfloat16)
        rot_ref[at // 2, queries:, :] = jnp.where(is_bias, far_below, 0.0).astype(jnp.bfloat16)

    def visit(block, masked):
        span = per * 2 * NOPE_DIM
        work = [(pair, i) for pair in range(pairs) for i in range(len(tiles))]
        shrinks = {}

        def expand_keys(n):
            key_refs[n][...] = jnp.dot(
                lat_ref[block],
                key_up_ref[:, n * span : (n + 1) * span],
                preferred_element_type=jnp.float32,
            ).astype(jnp.bfloat16)

        def expand_values(n):
            values = lax.dot_general(
                value_up_ref[n * span : (n + 1) * span, :],
                lat_ref[block],
                (((1,), (1,)), ((), ())),
                preferred_element_type=jnp.float32,
            ).astype(jnp.bfloat16)
            for head in range(2 * per):
                values_refs[n][head * head_rows : head * head_rows + VALUE_DIM, :] = values[
                    head * VALUE_DIM : (head + 1) * VALUE_DIM, :
                ]

        def product(at):
            pair, i = work[at]
            begin = tiles[i][0]
            within = (pair % per) * 2 * NOPE_DIM
            key_pair = jnp.concatenate(
                [key_refs[pair // per][:, within : within + 2 * NOPE_DIM], rot_ref[block]], axis=1
            )
            score = jnp.dot(
                key_pair, qbd_ref[pair, :, begin : begin + width], preferred_element_type=jnp.float32
            )
            if masked:
                column = lax.broadcasted_iota(jnp.int32, (queries, width), 1) + begin
                column = jnp.where(column >= queries, column - queries, column)
                visible = lax.broadcasted_iota(jnp.int32, (queries, width), 0) <= column
                score_refs[at % 2][:queries, :] = jnp.where(visible, score[:queries], far_below)
                score_refs[at % 2][queries:, :] = score[queries:]
            else:
                score_refs[at % 2][...] = score

        def soften(at):
            old_max = max_ref[at : at + 1, :]
            score = score_refs[at % 2]
            new_max = jnp.maximum(old_max, jnp.max(score[...], axis=0, keepdims=True))
            weight_refs[at % 2][...] = jnp.exp2(score[...] - new_max).astype(jnp.bfloat16)
            shrinks[at] = jnp.exp2(old_max - new_max)
            max_ref[at : at + 1, :] = new_max

        def weigh(at):
            pair, i = work[at]
            parts = tiles[i][1]
            head = 2 * (pair % per) + parts[0][0]
            fresh = jnp.dot(
                values_refs[pair // per][head * head_rows : (head + len(parts)) * head_rows, :],
                weight_refs[at % 2][...],
                preferred_element_type=jnp.float32,
            )
            if len(parts) > 1:
                fresh = jnp.concatenate(
                    [
                        fresh[n * head_rows : (n + 1) * head_rows, low:high]
                        for n, (_, low, high) in enumerate(parts)
                    ],
                    axis=1,
                )
            acc_ref[at] = acc_ref[at] * shrinks[at] + fresh

        share = per * len(tiles)
        expand_keys(0)
        product(0)
        expand_values(0)
        for at in range(len(work) + 1):
            ahead = (at + 3) // share
            if (at + 3) % share == 0 and 0 < ahead < parcels:
                expand_keys(ahead)
            ahead = (at + 1) // share
            if (at + 1) % share == 0 and 0 < ahead < parcels:
                expand_values(ahead)
            if at + 1 < len(work):
                product(at + 1)
            if at < len(work):
                soften(at)
            if at > 0:
                weigh(at - 1)

    if first:
        visit(0, True)

    @pl.loop(1 if first else 0, blocks)
    def each_block(block):
        low = 2 * block - (1 if first else 0)
        high = jnp.minimum(low + 1, slot - 1)

        @pl.when((vis_ref[low] > 0) | (vis_ref[high] > 0))
        def seen():
            visit(block, False)

    if last:
        for pair in range(pairs):
            pieces_of = ([], [])
            for i, (_, parts) in enumerate(tiles):
                done = acc_ref[pair * len(tiles) + i]
                done = done[:VALUE_DIM] / done[VALUE_DIM : VALUE_DIM + 1]
                for side, low, high in parts:
                    pieces_of[side].append(done[:, low:high])
            both = jnp.concatenate([jnp.concatenate(p, axis=1) for p in pieces_of], axis=0)
            out_ref[:, pair * 2 * VALUE_DIM : (pair + 1) * 2 * VALUE_DIM] = both.T.astype(out_ref.dtype)


def attention_stage(visible, queries_t, query_rot_t, key_up, value_up, slots, rows, groups,
                    order, own=None, state=None, last=False):
    first = own is not None
    heads = key_up.shape[1] // NOPE_DIM
    tok_rows = queries_t.shape[1]
    counts = [[p.shape[0] if p.ndim == 3 else 0 for p in s] for s in slots]
    total_blocks = sum(c[0] or 1 for c in counts) + (1 if first else 0)
    blocks = (total_blocks + 1) // 2
    width, tiles = tiles_of(tok_rows)
    tile_count = heads // 2 * len(tiles)
    extra = own if first else state
    consts = [queries_t, query_rot_t, key_up, value_up]
    flat = [p for s in slots for p in s]
    acc_shape = (tile_count, VALUE_DIM + SUM_ROWS, width)
    max_shape = (tile_count, width)
    parcels = max(1, heads // 4)
    keys = 2 * tok_rows
    scratch = (
        [
            pltpu.VMEM((blocks, keys, key_up.shape[0]), jnp.bfloat16),
            pltpu.VMEM((blocks, keys, 128), jnp.bfloat16),
            pltpu.VMEM((heads // 2, 256, 2 * tok_rows), jnp.bfloat16),
        ]
        + [pltpu.VMEM((keys, width), jnp.float32)] * 2
        + [pltpu.VMEM((keys, width), jnp.bfloat16)] * 2
        + [pltpu.VMEM((keys, heads // parcels * NOPE_DIM), jnp.bfloat16)] * parcels
        + [pltpu.VMEM((heads // parcels * (VALUE_DIM + SUM_ROWS), keys), jnp.bfloat16)] * parcels
    )
    if last:
        out_shape = jax.ShapeDtypeStruct((tok_rows, heads * VALUE_DIM), jnp.bfloat16)
        scratch = [pltpu.VMEM(max_shape, jnp.float32), pltpu.VMEM(acc_shape, jnp.float32)] + scratch
    else:
        out_shape = (
            jax.ShapeDtypeStruct(max_shape, jnp.float32),
            jax.ShapeDtypeStruct(acc_shape, jnp.float32),
        )
    flops = 2 * total_blocks * tok_rows * tok_rows * heads * (256 + VALUE_DIM)
    in_vmem = pl.BlockSpec()
    return pl.pallas_call(
        functools.partial(attention_kernel, first, last, counts, order, rows, groups, heads),
        in_specs=[pl.BlockSpec(memory_space=pltpu.SMEM)] + [in_vmem] * (len(consts) + len(flat) + len(extra)),
        out_specs=in_vmem if last else (in_vmem, in_vmem),
        scratch_shapes=scratch,
        out_shape=out_shape,
        compiler_params=pltpu.CompilerParams(vmem_limit_bytes=24 * 1024 * 1024),
        cost_estimate=pl.CostEstimate(
            flops=flops, bytes_accessed=4 << 20, transcendentals=total_blocks * tok_rows * tok_rows * heads
        ),
        name="attention_first" if first else "attention_rest",
    )(visible, *consts, *flat, *extra)


def conv_kernel(rim, gated_ref, rim_ref, taps_ref, out_ref, padded_ref):
    rows, chans = gated_ref.shape
    padded_ref[:rim, :] = rim_ref[...].astype(jnp.float32)
    padded_ref[rim : rim + rows, :] = gated_ref[...].astype(jnp.float32)
    offset = rim - (KERNEL - 1)
    step = math.gcd(rows, 64)
    for lane in range(0, chans, 128):
        lanes = slice(lane, lane + 128)
        for row in range(0, rows, step):
            acc = jnp.zeros((step, 128), jnp.float32)
            for phase in range(8):
                taps = range(phase, KERNEL, 8)
                start = row + offset + phase
                part = padded_ref[start : start + step + 8 * (len(taps) - 1), lanes]
                for j, tap in enumerate(taps):
                    acc = acc + taps_ref[tap : tap + 1, lanes] * part[8 * j : 8 * j + step]
            out_ref[row : row + step, lanes] = acc


def convolve(gated, rim, taps):
    rows, chans = gated.shape
    rim_rows = rim.shape[0]
    return pl.pallas_call(
        functools.partial(conv_kernel, rim_rows),
        out_shape=jax.ShapeDtypeStruct((rows, chans), jnp.float32),
        scratch_shapes=[pltpu.VMEM((rim_rows + rows, chans), jnp.float32)],
        compiler_params=pltpu.CompilerParams(vmem_limit_bytes=6 * 1024 * 1024),
        cost_estimate=pl.CostEstimate(
            flops=2 * KERNEL * rows * chans * 50, bytes_accessed=6 * rows * chans, transcendentals=0
        ),
        name="conv",
    )(gated, rim, taps)


def shards(
    tokens,
    input_gain,
    query_weight,
    query_rot_weight,
    kv_down,
    rot_down,
    kv_gain,
    key_up,
    value_up,
    conv_value_weight,
    conv_gate_weight,
    conv_taps,
    conv_ln_gain,
    conv_ln_bias,
    att_out_gain,
    conv_out_gain,
    att_out_weight,
    conv_out_weight,
):
    tok_rows = tokens.shape[0]
    heads_here = key_up.shape[1] // NOPE_DIM
    tp_size, sp_size = lax.axis_size("tp"), lax.axis_size("sp")
    tp_index, sp_index = lax.axis_index("tp"), lax.axis_index("sp")
    f32, bf16 = jnp.float32, jnp.bfloat16

    positions = sp_index * tok_rows + jnp.arange(tok_rows, dtype=jnp.int32)
    cos_table, sine_table = rotary_tables(positions, ROT_DIM // 2)

    rows = tok_rows // tp_size
    rank = kv_down.shape[1]
    groups = max(
        g for g in range(1, rank // ROT_DIM + 1) if rows % g == 0 and (rows // g) % 8 == 0
    )

    def near_by(array):
        return jnp.maximum(array, jnp.finfo(array.dtype).min)

    token_pieces = others(tokens, "tp")
    key_up = near_by(key_up)
    value_up = value_up.T
    scaled, row_scale, latent, own_rot, mine = front(
        jnp.full((1,), tp_index, jnp.int32),
        [near_by(tokens)] + token_pieces,
        near_by(input_gain)[None, :],
        near_by(kv_down),
        near_by(rot_down.T),
        near_by(kv_gain)[None, :],
        jnp.concatenate([cos_table, cos_table], axis=1),
        jnp.concatenate([-sine_table, sine_table], axis=1),
        groups,
    )

    plane = 4 if sp_size % 4 == 0 else 1
    high, low = sp_index // plane, sp_index % plane
    far = range(1, sp_size // plane)
    column = []
    for s in far:
        column.append(shift_by(mine, "sp", plane * s))
    column_vis = [(high >= s).astype(jnp.int32) for s in far]

    def with_pieces(arrays):
        return [[a] + others(a, "tp") for a in arrays]

    def project(weight):
        return jnp.dot(scaled, weight, preferred_element_type=f32)

    gated = (
        project(conv_value_weight) * row_scale * jax.nn.sigmoid(project(conv_gate_weight) * row_scale)
    ).astype(bf16)
    rim_rows = 32
    rim = shift_by(gated[tok_rows - rim_rows :], "sp", 1)
    scaled, gated = lax.optimization_barrier((scaled, gated))
    query_scale = row_scale * (math.log2(math.e) / math.sqrt(NOPE_DIM + ROT_DIM))
    queries_t = (project(query_weight) * query_scale).astype(bf16).T
    query_rot_t = (
        rotate_half(
            (project(query_rot_weight) * query_scale).reshape(tok_rows, heads_here, ROT_DIM),
            cos_table[:, None, :],
            sine_table[:, None, :],
        )
        .astype(bf16)
        .reshape(tok_rows, heads_here * ROT_DIM)
        .T
    )
    gated, rim, queries_t, query_rot_t = lax.optimization_barrier((gated, rim, queries_t, query_rot_t))
    conv_out = convolve(gated, rim, conv_taps)
    moments = total(jnp.stack([jnp.sum(conv_out, axis=1), jnp.sum(conv_out * conv_out, axis=1)]), "tp")
    mean_val = moments[0] / CONV_CH
    spread = moments[1] / CONV_CH - mean_val * mean_val
    normed = (conv_out - mean_val[:, None]) * lax.rsqrt(spread + norm_eps)[:, None]
    swished = jax.nn.silu(normed * conv_ln_gain[None, :] + conv_ln_bias[None, :])
    conv_sq = total(jnp.sum(swished * swished, axis=1)[None, :], "tp")[0]
    conv_mixed = (
        swished * lax.rsqrt(conv_sq / CONV_CH + norm_eps)[:, None] * conv_out_gain[None, :]
    ).astype(bf16)
    width = D_MODEL // tp_size

    def columns_of(device, weight):
        return lax.dynamic_slice_in_dim(weight, device * width, width, 1)

    def scatter(product):
        parts = []
        for d in range(1, tp_size):
            send = product((tp_index + tp_size - d) % tp_size).astype(bf16)
            parts.append(
                lax.ppermute(send, "tp", [((i + d) % tp_size, i) for i in range(tp_size)])
            )
        own = lax.optimization_barrier(product(tp_index))
        return own, parts

    own = (latent, own_rot)
    stage = functools.partial(
        attention_stage,
        queries_t=queries_t,
        query_rot_t=query_rot_t,
        key_up=key_up,
        value_up=value_up,
        rows=rows,
        groups=groups,
    )
    state = None
    arrived, vis_rest, order_rest = [], [], []
    slots, vis, order = with_pieces(column), column_vis, [(n, 0) for n in range(len(column))]
    if plane == 4:
        column_all = jnp.stack([mine] + column)
        for b in range(1, plane):
            arrived.append(swap_bits(column_all, "sp", b))
        for s in range(len(column) + 1):
            for b in range(1, plane):
                order_rest.append((b - 1, s))
                vis_rest.append(column_vis[s - 1] if s else ((low ^ b) < low).astype(jnp.int32))
        if slots:
            state = stage(jnp.stack(vis), slots=slots, order=order, own=own)
            state, arrived, conv_mixed = lax.optimization_barrier((state, arrived, conv_mixed))
        slots, vis, order = with_pieces(arrived), vis_rest, order_rest
    conv_own, conv_rest = scatter(
        lambda device: jnp.dot(
            conv_mixed, columns_of(device, conv_out_weight), preferred_element_type=f32
        )
    )
    conv_part = conv_own
    for part in conv_rest:
        conv_part = conv_part + part.astype(f32)
    if state is not None:
        state, conv_part = lax.optimization_barrier((state, conv_part))
        attended = stage(jnp.stack(vis), slots=slots, order=order, state=state, last=True)
    else:
        attended = stage(jnp.stack(vis), slots=slots, order=order, own=own, last=True)

    wide_att = attended.astype(f32)
    att_sq = total(jnp.sum(wide_att * wide_att, axis=1)[None, :], "tp")[0]
    gained = (wide_att * att_out_gain[None, :]).astype(bf16)
    att_part, att_rest = scatter(
        lambda device: jnp.dot(gained, columns_of(device, att_out_weight), preferred_element_type=f32)
    )
    for part in att_rest:
        att_part = att_part + part.astype(f32)
    return (att_part * lax.rsqrt(att_sq / ATT_WIDTH + norm_eps)[:, None] + conv_part).astype(bf16)


def solution(mesh):
    return jax.shard_map(
        shards,
        mesh=mesh,
        in_specs=(
            P("sp", "tp"),
            P(),
            P(None, "tp"),
            P(None, "tp"),
            P(),
            P(),
            P(),
            P(None, "tp"),
            P(None, "tp"),
            P(None, "tp"),
            P(None, "tp"),
            P(None, "tp"),
            P("tp"),
            P("tp"),
            P("tp"),
            P("tp"),
            P("tp", None),
            P("tp", None),
        ),
        out_specs=P("sp", "tp"),
        check_vma=False,
    )
```

```python
import functools
import math

import jax
import jax.numpy as jnp
from jax import lax
from jax.experimental import pallas as pl
from jax.experimental.pallas import tpu as pltpu
from jax.sharding import PartitionSpec as P


D_MODEL = 2048
NOPE_DIM = 64
ROT_DIM = 32
VALUE_DIM = 64
CONV_CH = 1024
KERNEL = 31
ATT_WIDTH = 1024


norm_eps = 1e-06
far_below = -1e30
rope_base = 10000.0
SUM_ROWS = 16


def rotary_tables(positions, half_dim):
    frequency = rope_base ** (-jnp.arange(half_dim, dtype=jnp.float32) / half_dim)
    angles = positions.astype(jnp.float32)[:, None] * frequency[None, :]
    return (jnp.cos(angles), jnp.sin(angles))


def rotate_half(values, cos_table, sine_table):
    half_dim = cos_table.shape[-1]
    front_half = values[..., :half_dim]
    back_half = values[..., half_dim:]
    return jnp.concatenate(
        [
            front_half * cos_table - back_half * sine_table,
            back_half * cos_table + front_half * sine_table,
        ],
        axis=-1,
    )


def shift_by(block, axis, distance):
    devices = range(lax.axis_size(axis))
    return lax.ppermute(block, axis, [(i, i + distance) for i in devices if i + distance in devices])


def swap_bits(block, axis, bits):
    return lax.ppermute(block, axis, [(i, i ^ bits) for i in range(lax.axis_size(axis))])


def others(block, axis):
    size = lax.axis_size(axis)
    return [
        lax.ppermute(block, axis, [((i + d) % size, i) for i in range(size)])
        for d in range(1, size)
    ]


def total(block, axis):
    for part in others(block, axis):
        block = block + part
    return block


def front_kernel(pieces, rows, groups, index_ref, *refs):
    token_refs, refs = refs[:pieces], refs[pieces:]
    gain_ref, down_ref, rot_down_ref, kv_gain_ref, cos_ref, sin_ref = refs[:6]
    scaled_ref, scale_ref, lat_ref, rot_ref, send_ref, wide_rot_ref = refs[6:]
    me = index_ref[0]
    tok_rows, width = token_refs[0].shape
    squares = jnp.zeros((tok_rows, 128), jnp.float32)
    for d, ref in enumerate(token_refs):
        begin = lax.rem(me + d, pieces) * width
        for col in range(0, width, 128):
            at = pl.ds(pl.multiple_of(begin + col, 128), 128)
            values = ref[:, col : col + 128].astype(jnp.float32)
            scaled_ref[:, at] = (values * gain_ref[:, at]).astype(jnp.bfloat16)
            squares = squares + values * values
    row_scale = lax.rsqrt(jnp.sum(squares, axis=1, keepdims=True) / D_MODEL + norm_eps)
    scale_ref[...] = row_scale
    raw = jnp.dot(scaled_ref[...], down_ref[...], preferred_element_type=jnp.float32)
    half = ROT_DIM // 2
    turned = jnp.concatenate(
        [rot_down_ref[...], rot_down_ref[half:, :], rot_down_ref[:half, :]], axis=0
    )
    both = (
        lax.dot_general(
            scaled_ref[...], turned, (((1,), (1,)), ((), ())), preferred_element_type=jnp.float32
        )
        * row_scale
    )
    mean = jnp.mean(raw * raw, axis=1, keepdims=True)
    lat_ref[...] = (raw * lax.rsqrt(mean + norm_eps) * kv_gain_ref[...]).astype(jnp.bfloat16)
    rot = both[:, :ROT_DIM] * cos_ref[...] + both[:, ROT_DIM : 2 * ROT_DIM] * sin_ref[...]
    rot = jnp.concatenate([rot, jnp.zeros((tok_rows, 128 - ROT_DIM), jnp.float32)], axis=1)
    wide_rot_ref[...] = rot
    rot_ref[...] = rot.astype(jnp.bfloat16)
    start = me * rows
    send_ref[:rows, :] = lat_ref[pl.ds(pl.multiple_of(start, 16), rows), :]
    height = rows // groups
    packed = [
        wide_rot_ref[pl.ds(pl.multiple_of(start + g * height, 8), height), :][:, :ROT_DIM]
        for g in range(groups)
    ]
    rank = lat_ref.shape[1]
    if groups * ROT_DIM < rank:
        packed.append(jnp.zeros((height, rank - groups * ROT_DIM), jnp.float32))
    packed = jnp.concatenate(packed, axis=1)
    spare = send_ref.shape[0] - rows - height
    if spare:
        packed = jnp.concatenate([packed, jnp.zeros((spare, rank), jnp.float32)], axis=0)
    send_ref[rows:, :] = packed.astype(jnp.bfloat16)


def front(index, pieces, gain, down, rot_down, kv_gain, cos, sin, groups):
    tok_rows, width = pieces[0].shape
    rank = down.shape[1]
    rows = tok_rows // len(pieces)
    height = rows // groups
    model = width * len(pieces)
    in_vmem = pl.BlockSpec()
    args = list(pieces) + [gain, down, rot_down, kv_gain, cos, sin]
    return pl.pallas_call(
        functools.partial(front_kernel, len(pieces), rows, groups),
        in_specs=[pl.BlockSpec(memory_space=pltpu.SMEM)] + [in_vmem] * len(args),
        out_specs=(in_vmem,) * 5,
        out_shape=(
            jax.ShapeDtypeStruct((tok_rows, model), jnp.bfloat16),
            jax.ShapeDtypeStruct((tok_rows, 1), jnp.float32),
            jax.ShapeDtypeStruct((tok_rows, rank), jnp.bfloat16),
            jax.ShapeDtypeStruct((tok_rows, 128), jnp.bfloat16),
            jax.ShapeDtypeStruct((rows + height + -height % 16, rank), jnp.bfloat16),
        ),
        scratch_shapes=[pltpu.VMEM((tok_rows, 128), jnp.float32)],
        compiler_params=pltpu.CompilerParams(vmem_limit_bytes=16 * 1024 * 1024),
        cost_estimate=pl.CostEstimate(
            flops=2 * tok_rows * model * 512, bytes_accessed=8 << 20, transcendentals=tok_rows
        ),
        name="front",
    )(index, *args)


def tiles_of(queries):
    width = 256 if (2 * queries) % 256 == 0 else queries
    out = []
    for start in range(0, 2 * queries, width):
        parts = []
        for side in range(2):
            low = max(start, side * queries)
            high = min(start + width, (side + 1) * queries)
            if low < high:
                parts.append((side, low - start, high - start))
        out.append((start, parts))
    return width, out


def attention_kernel(first, last, counts, order, rows, groups, heads, vis_ref, *refs):
    refs = list(refs)
    qt_ref, qrt_ref, key_up_ref, value_up_ref = refs[:4]
    refs = refs[4:]
    pieces = len(counts[0])
    sources = []
    for _ in counts:
        sources.append(refs[:pieces])
        refs = refs[pieces:]
    if first:
        (own_lat_ref, own_rot_ref), refs = refs[:2], refs[2:]
    else:
        (max_in, acc_in), refs = refs[:2], refs[2:]
    if last:
        (out_ref, max_ref, acc_ref), refs = refs[:3], refs[3:]
    else:
        (max_ref, acc_ref), refs = refs[:2], refs[2:]
    lat_ref, rot_ref, qbd_ref, turned_ref, score_refs, weight_refs, refs = (
        refs[0], refs[1], refs[2], refs[3], refs[4:6], refs[6:8], refs[8:]
    )
    pairs = heads // 2
    parcels = max(1, pairs // 2)
    key_refs, values_refs = refs[:parcels], refs[parcels:]
    per = pairs // parcels
    queries = qt_ref.shape[1]
    width, tiles = tiles_of(queries)
    head_rows = VALUE_DIM + SUM_ROWS
    blocks = lat_ref.shape[0]
    bias_row = 2 * NOPE_DIM + ROT_DIM

    turned_ref[...] = value_up_ref[...].T
    qbd_ref[...] = jnp.zeros_like(qbd_ref)
    for pair in range(pairs):
        qbd_ref[pair, bias_row : bias_row + 16, :] = (
            lax.broadcasted_iota(jnp.int32, (16, 2 * queries), 0) == 0
        ).astype(jnp.bfloat16)
        for side in range(2):
            head = 2 * pair + side
            columns = slice(side * queries, (side + 1) * queries)
            qbd_ref[pair, side * NOPE_DIM : (side + 1) * NOPE_DIM, columns] = qt_ref[
                head * NOPE_DIM : (head + 1) * NOPE_DIM, :
            ]
            qbd_ref[pair, 2 * NOPE_DIM : 2 * NOPE_DIM + ROT_DIM, columns] = qrt_ref[
                head * ROT_DIM : (head + 1) * ROT_DIM, :
            ]
    for ref in values_refs:
        ref[...] = jnp.ones_like(ref)
    if first:
        max_ref[...] = jnp.full_like(max_ref, far_below)
        acc_ref[...] = jnp.zeros_like(acc_ref)
        lat_ref[0, :queries, :] = own_lat_ref[...]
        rot_ref[0, :queries, :] = own_rot_ref[...]
    else:
        max_ref[...] = max_in[...]
        acc_ref[...] = acc_in[...]

    at = 1 if first else 0
    slot = 0
    is_bias = lax.broadcasted_iota(jnp.int32, (queries, 128), 1) == ROT_DIM
    for place, index in order:
        rots = []
        base = (at % 2) * queries
        for n, ref in enumerate(sources[place]):
            view = ref.at[index] if counts[place][0] else ref
            lat_ref[at // 2, base + n * rows : base + (n + 1) * rows, :] = view[:rows, :]
            packed = view[rows:, :].astype(jnp.float32)[: rows // groups]
            rots += [packed[:, g * ROT_DIM : (g + 1) * ROT_DIM] for g in range(groups)]
        rot = jnp.concatenate(rots, axis=0)
        rot = jnp.concatenate([rot, jnp.zeros((queries, 128 - ROT_DIM), jnp.float32)], axis=1)
        bias = jnp.where(vis_ref[slot] > 0, 0.0, far_below)
        rot_ref[at // 2, base : base + queries, :] = jnp.where(is_bias, bias, rot).astype(jnp.bfloat16)
        at += 1
        slot += 1
    if at % 2:
        lat_ref[at // 2, queries:, :] = jnp.zeros((queries, lat_ref.shape[2]), jnp.bfloat16)
        rot_ref[at // 2, queries:, :] = jnp.where(is_bias, far_below, 0.0).astype(jnp.bfloat16)

    def visit(block, masked):
        span = per * 2 * NOPE_DIM
        work = [(pair, i) for pair in range(pairs) for i in range(len(tiles))]
        shrinks = {}

        def expand_keys(n):
            key_refs[n][...] = jnp.dot(
                lat_ref[block],
                key_up_ref[:, n * span : (n + 1) * span],
                preferred_element_type=jnp.float32,
            ).astype(jnp.bfloat16)

        def expand_values(n):
            values = lax.dot_general(
                turned_ref[n * span : (n + 1) * span, :],
                lat_ref[block],
                (((1,), (1,)), ((), ())),
                preferred_element_type=jnp.float32,
            ).astype(jnp.bfloat16)
            for head in range(2 * per):
                values_refs[n][head * head_rows : head * head_rows + VALUE_DIM, :] = values[
                    head * VALUE_DIM : (head + 1) * VALUE_DIM, :
                ]

        def product(at):
            pair, i = work[at]
            begin = tiles[i][0]
            within = (pair % per) * 2 * NOPE_DIM
            key_pair = jnp.concatenate(
                [key_refs[pair // per][:, within : within + 2 * NOPE_DIM], rot_ref[block]], axis=1
            )
            score = jnp.dot(
                key_pair, qbd_ref[pair, :, begin : begin + width], preferred_element_type=jnp.float32
            )
            if masked:
                column = lax.broadcasted_iota(jnp.int32, (queries, width), 1) + begin
                column = jnp.where(column >= queries, column - queries, column)
                visible = lax.broadcasted_iota(jnp.int32, (queries, width), 0) <= column
                score_refs[at % 2][:queries, :] = jnp.where(visible, score[:queries], far_below)
                score_refs[at % 2][queries:, :] = score[queries:]
            else:
                score_refs[at % 2][...] = score

        def soften(at):
            old_max = max_ref[at : at + 1, :]
            score = score_refs[at % 2]
            new_max = jnp.maximum(old_max, jnp.max(score[...], axis=0, keepdims=True))
            weight_refs[at % 2][...] = jnp.exp2(score[...] - new_max).astype(jnp.bfloat16)
            shrinks[at] = jnp.exp2(old_max - new_max)
            max_ref[at : at + 1, :] = new_max

        def weigh(at):
            pair, i = work[at]
            parts = tiles[i][1]
            head = 2 * (pair % per) + parts[0][0]
            fresh = jnp.dot(
                values_refs[pair // per][head * head_rows : (head + len(parts)) * head_rows, :],
                weight_refs[at % 2][...],
                preferred_element_type=jnp.float32,
            )
            if len(parts) > 1:
                fresh = jnp.concatenate(
                    [
                        fresh[n * head_rows : (n + 1) * head_rows, low:high]
                        for n, (_, low, high) in enumerate(parts)
                    ],
                    axis=1,
                )
            acc_ref[at] = acc_ref[at] * shrinks[at] + fresh

        share = per * len(tiles)
        expand_keys(0)
        product(0)
        expand_values(0)
        for at in range(len(work) + 1):
            ahead = (at + 3) // share
            if (at + 3) % share == 0 and 0 < ahead < parcels:
                expand_keys(ahead)
            ahead = (at + 1) // share
            if (at + 1) % share == 0 and 0 < ahead < parcels:
                expand_values(ahead)
            if at + 1 < len(work):
                product(at + 1)
            if at < len(work):
                soften(at)
            if at > 0:
                weigh(at - 1)

    if first:
        visit(0, True)

    @pl.loop(1 if first else 0, blocks)
    def each_block(block):
        low = 2 * block - (1 if first else 0)
        high = jnp.minimum(low + 1, slot - 1)

        @pl.when((vis_ref[low] > 0) | (vis_ref[high] > 0))
        def seen():
            visit(block, False)

    if last:
        for pair in range(pairs):
            pieces_of = ([], [])
            for i, (_, parts) in enumerate(tiles):
                done = acc_ref[pair * len(tiles) + i]
                done = done[:VALUE_DIM] / done[VALUE_DIM : VALUE_DIM + 1]
                for side, low, high in parts:
                    pieces_of[side].append(done[:, low:high])
            both = jnp.concatenate([jnp.concatenate(p, axis=1) for p in pieces_of], axis=0)
            out_ref[:, pair * 2 * VALUE_DIM : (pair + 1) * 2 * VALUE_DIM] = both.T.astype(out_ref.dtype)


def attention_stage(visible, queries_t, query_rot_t, key_up, value_up, slots, rows, groups,
                    order, own=None, state=None, last=False):
    first = own is not None
    heads = key_up.shape[1] // NOPE_DIM
    tok_rows = queries_t.shape[1]
    counts = [[p.shape[0] if p.ndim == 3 else 0 for p in s] for s in slots]
    total_blocks = sum(c[0] or 1 for c in counts) + (1 if first else 0)
    blocks = (total_blocks + 1) // 2
    width, tiles = tiles_of(tok_rows)
    tile_count = heads // 2 * len(tiles)
    extra = own if first else state
    consts = [queries_t, query_rot_t, key_up, value_up]
    flat = [p for s in slots for p in s]
    acc_shape = (tile_count, VALUE_DIM + SUM_ROWS, width)
    max_shape = (tile_count, width)
    parcels = max(1, heads // 4)
    keys = 2 * tok_rows
    scratch = (
        [
            pltpu.VMEM((blocks, keys, key_up.shape[0]), jnp.bfloat16),
            pltpu.VMEM((blocks, keys, 128), jnp.bfloat16),
            pltpu.VMEM((heads // 2, 256, 2 * tok_rows), jnp.bfloat16),
            pltpu.VMEM(value_up.shape[::-1], jnp.bfloat16),
        ]
        + [pltpu.VMEM((keys, width), jnp.float32)] * 2
        + [pltpu.VMEM((keys, width), jnp.bfloat16)] * 2
        + [pltpu.VMEM((keys, heads // parcels * NOPE_DIM), jnp.bfloat16)] * parcels
        + [pltpu.VMEM((heads // parcels * (VALUE_DIM + SUM_ROWS), keys), jnp.bfloat16)] * parcels
    )
    if last:
        out_shape = jax.ShapeDtypeStruct((tok_rows, heads * VALUE_DIM), jnp.bfloat16)
        scratch = [pltpu.VMEM(max_shape, jnp.float32), pltpu.VMEM(acc_shape, jnp.float32)] + scratch
    else:
        out_shape = (
            jax.ShapeDtypeStruct(max_shape, jnp.float32),
            jax.ShapeDtypeStruct(acc_shape, jnp.float32),
        )
    flops = 2 * total_blocks * tok_rows * tok_rows * heads * (256 + VALUE_DIM)
    in_vmem = pl.BlockSpec()
    return pl.pallas_call(
        functools.partial(attention_kernel, first, last, counts, order, rows, groups, heads),
        in_specs=[pl.BlockSpec(memory_space=pltpu.SMEM)] + [in_vmem] * (len(consts) + len(flat) + len(extra)),
        out_specs=in_vmem if last else (in_vmem, in_vmem),
        scratch_shapes=scratch,
        out_shape=out_shape,
        compiler_params=pltpu.CompilerParams(vmem_limit_bytes=24 * 1024 * 1024),
        cost_estimate=pl.CostEstimate(
            flops=flops, bytes_accessed=4 << 20, transcendentals=total_blocks * tok_rows * tok_rows * heads
        ),
        name="attention_first" if first else "attention_rest",
    )(visible, *consts, *flat, *extra)


def conv_kernel(rim, gated_ref, rim_ref, taps_ref, out_ref, padded_ref):
    rows, chans = gated_ref.shape
    padded_ref[:rim, :] = rim_ref[...].astype(jnp.float32)
    padded_ref[rim : rim + rows, :] = gated_ref[...].astype(jnp.float32)
    offset = rim - (KERNEL - 1)
    step = math.gcd(rows, 64)
    for lane in range(0, chans, 128):
        lanes = slice(lane, lane + 128)
        for row in range(0, rows, step):
            acc = jnp.zeros((step, 128), jnp.float32)
            for phase in range(8):
                taps = range(phase, KERNEL, 8)
                start = row + offset + phase
                part = padded_ref[start : start + step + 8 * (len(taps) - 1), lanes]
                for j, tap in enumerate(taps):
                    acc = acc + taps_ref[tap : tap + 1, lanes] * part[8 * j : 8 * j + step]
            out_ref[row : row + step, lanes] = acc


def convolve(gated, rim, taps):
    rows, chans = gated.shape
    rim_rows = rim.shape[0]
    return pl.pallas_call(
        functools.partial(conv_kernel, rim_rows),
        out_shape=jax.ShapeDtypeStruct((rows, chans), jnp.float32),
        scratch_shapes=[pltpu.VMEM((rim_rows + rows, chans), jnp.float32)],
        compiler_params=pltpu.CompilerParams(vmem_limit_bytes=6 * 1024 * 1024),
        cost_estimate=pl.CostEstimate(
            flops=2 * KERNEL * rows * chans * 50, bytes_accessed=6 * rows * chans, transcendentals=0
        ),
        name="conv",
    )(gated, rim, taps)


def shards(
    tokens,
    input_gain,
    query_weight,
    query_rot_weight,
    kv_down,
    rot_down,
    kv_gain,
    key_up,
    value_up,
    conv_value_weight,
    conv_gate_weight,
    conv_taps,
    conv_ln_gain,
    conv_ln_bias,
    att_out_gain,
    conv_out_gain,
    att_out_weight,
    conv_out_weight,
):
    tok_rows = tokens.shape[0]
    heads_here = key_up.shape[1] // NOPE_DIM
    tp_size, sp_size = lax.axis_size("tp"), lax.axis_size("sp")
    tp_index, sp_index = lax.axis_index("tp"), lax.axis_index("sp")
    f32, bf16 = jnp.float32, jnp.bfloat16

    positions = sp_index * tok_rows + jnp.arange(tok_rows, dtype=jnp.int32)
    cos_table, sine_table = rotary_tables(positions, ROT_DIM // 2)

    rows = tok_rows // tp_size
    rank = kv_down.shape[1]
    groups = max(
        g for g in range(1, rank // ROT_DIM + 1) if rows % g == 0 and (rows // g) % 8 == 0
    )

    def near_by(array):
        return jnp.maximum(array, jnp.finfo(array.dtype).min)

    token_pieces = others(tokens, "tp")
    key_up = near_by(key_up)
    value_up = near_by(value_up)
    scaled, row_scale, latent, own_rot, mine = front(
        jnp.full((1,), tp_index, jnp.int32),
        [near_by(tokens)] + token_pieces,
        near_by(input_gain)[None, :],
        near_by(kv_down),
        near_by(rot_down.T),
        near_by(kv_gain)[None, :],
        jnp.concatenate([cos_table, cos_table], axis=1),
        jnp.concatenate([-sine_table, sine_table], axis=1),
        groups,
    )

    plane = 4 if sp_size % 4 == 0 else 1
    high, low = sp_index // plane, sp_index % plane
    far = range(1, sp_size // plane)
    column = []
    for s in far:
        column.append(shift_by(mine, "sp", plane * s))
    column_vis = [(high >= s).astype(jnp.int32) for s in far]

    def with_pieces(arrays):
        return [[a] + others(a, "tp") for a in arrays]

    def project(weight):
        return jnp.dot(scaled, weight, preferred_element_type=f32)

    gated = (
        project(conv_value_weight) * row_scale * jax.nn.sigmoid(project(conv_gate_weight) * row_scale)
    ).astype(bf16)
    rim_rows = 32
    rim = shift_by(gated[tok_rows - rim_rows :], "sp", 1)
    scaled, gated = lax.optimization_barrier((scaled, gated))
    query_scale = row_scale * (math.log2(math.e) / math.sqrt(NOPE_DIM + ROT_DIM))
    queries_t = (project(query_weight) * query_scale).astype(bf16).T
    query_rot_t = (
        rotate_half(
            (project(query_rot_weight) * query_scale).reshape(tok_rows, heads_here, ROT_DIM),
            cos_table[:, None, :],
            sine_table[:, None, :],
        )
        .astype(bf16)
        .reshape(tok_rows, heads_here * ROT_DIM)
        .T
    )
    gated, rim, queries_t, query_rot_t = lax.optimization_barrier((gated, rim, queries_t, query_rot_t))
    conv_out = convolve(gated, rim, conv_taps)
    moments = total(jnp.stack([jnp.sum(conv_out, axis=1), jnp.sum(conv_out * conv_out, axis=1)]), "tp")
    mean_val = moments[0] / CONV_CH
    spread = moments[1] / CONV_CH - mean_val * mean_val
    normed = (conv_out - mean_val[:, None]) * lax.rsqrt(spread + norm_eps)[:, None]
    swished = jax.nn.silu(normed * conv_ln_gain[None, :] + conv_ln_bias[None, :])
    conv_sq = total(jnp.sum(swished * swished, axis=1)[None, :], "tp")[0]
    conv_mixed = (
        swished * lax.rsqrt(conv_sq / CONV_CH + norm_eps)[:, None] * conv_out_gain[None, :]
    ).astype(bf16)
    width = D_MODEL // tp_size

    def columns_of(device, weight):
        return lax.dynamic_slice_in_dim(weight, device * width, width, 1)

    def scatter(product):
        parts = []
        for d in range(1, tp_size):
            send = product((tp_index + tp_size - d) % tp_size).astype(bf16)
            parts.append(
                lax.ppermute(send, "tp", [((i + d) % tp_size, i) for i in range(tp_size)])
            )
        own = lax.optimization_barrier(product(tp_index))
        return own, parts

    own = (latent, own_rot)
    stage = functools.partial(
        attention_stage,
        queries_t=queries_t,
        query_rot_t=query_rot_t,
        key_up=key_up,
        value_up=value_up,
        rows=rows,
        groups=groups,
    )
    state = None
    arrived, vis_rest, order_rest = [], [], []
    slots, vis, order = with_pieces(column), column_vis, [(n, 0) for n in range(len(column))]
    if plane == 4:
        column_all = jnp.stack([mine] + column)
        for b in range(1, plane):
            arrived.append(swap_bits(column_all, "sp", b))
        for s in range(len(column) + 1):
            for b in range(1, plane):
                order_rest.append((b - 1, s))
                vis_rest.append(column_vis[s - 1] if s else ((low ^ b) < low).astype(jnp.int32))
        if slots:
            state = stage(jnp.stack(vis), slots=slots, order=order, own=own)
            state, arrived, conv_mixed = lax.optimization_barrier((state, arrived, conv_mixed))
        slots, vis, order = with_pieces(arrived), vis_rest, order_rest
    conv_own, conv_rest = scatter(
        lambda device: jnp.dot(
            conv_mixed, columns_of(device, conv_out_weight), preferred_element_type=f32
        )
    )
    conv_part = conv_own
    for part in conv_rest:
        conv_part = conv_part + part.astype(f32)
    if state is not None:
        state, conv_part = lax.optimization_barrier((state, conv_part))
        attended = stage(jnp.stack(vis), slots=slots, order=order, state=state, last=True)
    else:
        attended = stage(jnp.stack(vis), slots=slots, order=order, own=own, last=True)

    wide_att = attended.astype(f32)
    att_sq = total(jnp.sum(wide_att * wide_att, axis=1)[None, :], "tp")[0]
    gained = (wide_att * att_out_gain[None, :]).astype(bf16)
    att_part, att_rest = scatter(
        lambda device: jnp.dot(gained, columns_of(device, att_out_weight), preferred_element_type=f32)
    )
    for part in att_rest:
        att_part = att_part + part.astype(f32)
    return (att_part * lax.rsqrt(att_sq / ATT_WIDTH + norm_eps)[:, None] + conv_part).astype(bf16)


def solution(mesh):
    return jax.shard_map(
        shards,
        mesh=mesh,
        in_specs=(
            P("sp", "tp"),
            P(),
            P(None, "tp"),
            P(None, "tp"),
            P(),
            P(),
            P(),
            P(None, "tp"),
            P(None, "tp"),
            P(None, "tp"),
            P(None, "tp"),
            P(None, "tp"),
            P("tp"),
            P("tp"),
            P("tp"),
            P("tp"),
            P("tp", None),
            P("tp", None),
        ),
        out_specs=P("sp", "tp"),
        check_vma=False,
    )
```
